128 devices in a mesh: sp: 32 (over z, y, core), tp: 4 (over x).
Axes of the slice: x: 4, y: 4, z: 4, core: 2. Of those that a mesh axis runs over, the one named last changes fastest.
Arguments:
- queries: bfloat16 [16384, 1024], P('sp', 'tp'), may hold values from -6 to 6
- key_heads: bfloat16 [16384, 512], P('sp', 'tp'), may hold values from -6 to 6
- value_heads: bfloat16 [16384, 512], P('sp', 'tp'), may hold values from -70 to 70
- documents: int32 [16384], P('sp'), may hold values from 0 to 8, never falling along the last dimension, each value on 1 to 10240 neighbouring positions
- query_gain: float32 [128], replicated, may hold values from 0.1 to 8
- key_gain: float32 [128], replicated, may hold values from 0.1 to 8
- out_gain: float32 [1024], replicated, may hold values from 0.1 to 1.9
- out_proj: bfloat16 [1024, 2048], replicated, may hold values from -0.1875 to 0.1875
- residual: bfloat16 [16384, 2048], P(('sp', 'tp')), may hold values from -6 to 6
- mid_gain: float32 [2048], replicated, may hold values from 0.1 to 1.9
- mid_bias: float32 [2048], replicated, may hold values from -1.5 to 1.5
- routes: int32 [16384, 2], P(('sp', 'tp')), may hold values from 0 to 127, all different within a row; in each aligned block of 128 rows (0 to 127, 128 to 255, ...) at most 4 rows name the same one
- route_weights: float32 [16384, 2], P(('sp', 'tp')), may hold values from 0.2 to 2
- expert_gate: bfloat16 [128, 2048, 512], P(('sp', 'tp')), may hold values from -0.125 to 0.125
- expert_up: bfloat16 [128, 2048, 512], P(('sp', 'tp')), may hold values from -0.125 to 0.125
- expert_down: bfloat16 [128, 512, 2048], P(('sp', 'tp')), may hold values from -0.25 to 0.25
- final_gain: float32 [2048], replicated, may hold values from 0.1 to 1.9
- final_bias: float32 [2048], replicated, may hold values from -1.5 to 1.5
Outputs:
- layer_out: bfloat16 [16384, 2048], P(('sp', 'tp'))
The draws below stay inside these ranges and needn't reach their ends.
Inputs may be any that keep to these rules, and one draw needn't show every extreme that they name: `documents`: never falls along the sequence; each document holds 1 to 10240 positions and one holds exactly 10240. `routes`: each row names 2 different experts; among the rows of one device (aligned blocks of 128 rows) no expert is named more than 4 times, and exactly 4 times in some block.
All inputs are finite; a program needn't handle non-finite values.
Results may differ from the reference program's by a relative error of at most 0.014.
The reference program's roundings to bfloat16 on the way count: a program that leaves them out, or rounds other values in their place, can miss the bound.
Values may be sent and summed in bfloat16 or wider, within the bound.
No kernel may reach another device: no remote copies, remote signals or barrier semaphores. Data moves between devices by JAX's collectives and lax.ppermute only.
A program may use at most 128 MiB of HBM per device.

```python
import math
import jax
import jax.numpy as jnp
import numpy as np
from jax import lax

D = 2048
HEAD = 128
QH = 8
KVH = 4
GRID = 64
DE = 512
TOP_K = 2
TOKENS = 16384
ROWS = 128
EXPERTS = 128
CAP = 4
DOCS = 9
DOC_MOST = 10240
N_SP = 32
N_TP = 4


def drawn_keys(key):
    sub_key = jax.random.fold_in(key, 202)
    drawn = jnp.clip(jax.random.normal(sub_key, (TOKENS, KVH * HEAD), jnp.float32), -6.0, 6.0)
    return drawn


def draw_key_heads(key, part):
    return drawn_keys(key).astype(jnp.bfloat16)


def draw_queries(key, part):
    sub_key = jax.random.fold_in(key, 301)
    drawn = jnp.clip(jax.random.normal(sub_key, (TOKENS, QH * HEAD), jnp.float32), -6.0, 6.0)
    return drawn.astype(jnp.bfloat16)


def draw_value_heads(key, part):
    sub_key = jax.random.fold_in(key, 501)
    head_index = jnp.arange(KVH, dtype=jnp.float32)
    head_scale = jnp.repeat(4.0 ** (head_index / (KVH - 1)), HEAD)
    drawn = jnp.clip(jax.random.normal(sub_key, (TOKENS, KVH * HEAD), jnp.float32), -4.0, 4.0)
    return (drawn * head_scale[None, :]).astype(jnp.bfloat16)


def gain_values(key):
    return jnp.clip(1.0 + 0.18 * jax.random.normal(key, (HEAD,), jnp.float32), 0.1, 1.9)


def draw_query_gain(key, part):
    return gain_values(jax.random.fold_in(key, 401))


def draw_key_gain(key, part):
    return gain_values(jax.random.fold_in(key, 402))


def levels(stream_key, shape, shards, smallest, largest):
    loudness, own = 1.0, jax.random.fold_in(stream_key, 6)
    for position, shards_of in shards:
        heights = jnp.exp(jax.random.uniform(jax.random.fold_in(own, position), (shards_of,), jnp.float32, smallest / len(shards), largest / len(shards)))
        loudness = loudness * jnp.repeat(heights, shape[position] // shards_of).reshape([-1 if axis == position else 1 for axis in range(len(shape))])
    return loudness


def profile(amount, total, limit, skew):
    portions = [(1 << 20) // math.isqrt(rank ** skew) + 1 for rank in range(2, amount + 1)]
    surplus, holding = total - limit - (amount - 1), [1] * (amount - 1)
    while surplus > 0:
        movable = [i for i in range(amount - 1) if holding[i] < limit]
        whole, left = sum([portions[i] for i in movable]), surplus
        for i in movable:
            extra = min(limit - holding[i], max(1, left * portions[i] // whole), surplus)
            holding[i] = holding[i] + extra
            surplus = surplus - extra
    return np.array([limit] + holding)


def uneven_parts(rng, amount, total, limit, skew):
    if amount == 2:
        one = jax.random.randint(rng, (), max(1, total - limit), min(limit, total - 1) + 1)
        return jnp.stack([one, total - one])
    tallies = jnp.asarray(profile(amount, total, limit, skew), jnp.int32)
    twos = (amount - 1) // 2
    donor, taker = tallies[1:1 + 2 * twos:2], tallies[2:2 + 2 * twos:2]
    room = jnp.minimum(donor - 1, limit - taker)
    passed = jax.random.randint(jax.random.fold_in(rng, 1), (twos,), 0, 1 << 20) % (room + 1)
    tallies = tallies.at[1:1 + 2 * twos:2].set(donor - passed).at[2:2 + 2 * twos:2].set(taker + passed)
    return tallies[jax.random.permutation(jax.random.fold_in(rng, 2), amount)]


def assign_block(key, own, number, rows, number_of, top, limit, slope):
    order = jax.random.permutation(key, number_of)
    crowded, common = portions_of(number_of, rows * top, limit, slope, True), portions_of(number_of, rows * top, limit, slope, False)
    places = jnp.arange(number_of)

    def named(sizes, offset_by):
        used = int((sizes > 0).sum())
        fixed = max(1, used // 4)
        passed = fixed + (places - fixed + offset_by * (used - fixed)) % max(1, number_of - fixed)
        return jnp.zeros((number_of,), jnp.int32).at[order[jnp.where(places < fixed, places, passed)]].set(jnp.asarray(sizes, jnp.int32))

    sizes = jnp.where(number % 4 == 0, named(crowded, number // 4), named(common, number - number // 4 - 1))
    mixed = jax.random.permutation(jax.random.fold_in(own, 3), number_of)
    giver, receiver = mixed[0:number_of // 2 * 2:2], mixed[1:number_of // 2 * 2:2]
    slack = jnp.minimum(sizes[giver] - 1, limit - sizes[receiver]) // 2
    slack = jnp.where((giver == order[0]) | (receiver == order[0]) | (sizes[receiver] == 0), 0, jnp.maximum(slack, 0))
    passed = jax.random.randint(jax.random.fold_in(own, 4), (number_of // 2,), 0, 1 << 20) % (slack + 1)
    sizes = sizes.at[giver].add(-passed).at[receiver].add(passed)
    items = jnp.searchsorted(jnp.cumsum(sizes), jnp.arange(rows * top), side="right").astype(jnp.int32)
    table = items.reshape(top, rows).T
    table = table[jax.random.permutation(jax.random.fold_in(own, 1), rows)]
    offset_by = jax.random.randint(jax.random.fold_in(own, 2), (rows, 1), 0, top)
    return jnp.take_along_axis(table, (jnp.arange(top)[None, :] + offset_by) % top, axis=1)


def portions_of(amount, total, most, lean, full):
    loads = [(1 << 20) // math.isqrt(standing ** lean) + 1 for standing in range(1, amount + 1)]
    largest = most if full else min(most, max(-(-total // amount), total * loads[0] // sum(loads)))
    least = 1 if total - largest >= amount - 1 else 0
    given, spare = [largest] + [least] * (amount - 1), total - largest - least * (amount - 1)
    while spare > 0:
        candidates = [i for i in range(1, amount) if given[i] < largest] or [i for i in range(1, amount) if given[i] < most]
        mass, left = sum([loads[i] for i in candidates]), spare
        for i in candidates:
            extra = min(most - given[i], max(1, left * loads[i] // mass), spare)
            given[i] = given[i] + extra
            spare = spare - extra
    return np.array(given)


def gaussian(stream_key, extent, deviation, limit, shards=(), kind=jnp.bfloat16):
    array = deviation * jax.random.normal(stream_key, extent, jnp.float32)
    if shards:
        array = array * levels(stream_key, extent, shards, -0.22, 0.18)
    return jnp.clip(array, -limit, limit).astype(kind)


def setup_inputs(seed: int = 0) -> dict:
    streams_of = jax.random.split(jax.random.key(seed), 19)
    queries = draw_queries(jax.random.fold_in(streams_of[18], 71), 0)
    key_heads = draw_key_heads(jax.random.fold_in(streams_of[18], 71), 0)
    value_heads = draw_value_heads(jax.random.fold_in(streams_of[18], 71), 0)
    documents = jnp.searchsorted(jnp.cumsum(uneven_parts(streams_of[3], DOCS, TOKENS, DOC_MOST, 1)), jnp.arange(TOKENS), side="right").astype(jnp.int32)
    query_gain = draw_query_gain(jax.random.fold_in(streams_of[18], 71), 0)
    key_gain = draw_key_gain(jax.random.fold_in(streams_of[18], 71), 0)
    out_gain = jnp.clip(1.0 + 0.18 * jax.random.normal(streams_of[6], (QH * HEAD,), jnp.float32), 0.1, 1.9)
    out_proj = gaussian(streams_of[7], (QH * HEAD, D), (QH * HEAD) ** -0.5, 0.1875)
    residual = gaussian(streams_of[8], (TOKENS, D), 1.0, 6.0, ((0, 128),))
    mid_gain = jnp.clip(1.0 + 0.18 * jax.random.normal(streams_of[9], (D,), jnp.float32), 0.1, 1.9)
    mid_bias = gaussian(streams_of[10], (D,), 0.3, 1.5, (), jnp.float32)
    routes_keys = jax.random.split(jax.random.fold_in(streams_of[11], 1), TOKENS // ROWS)
    routes_turns = jax.random.permutation(jax.random.fold_in(streams_of[11], 3), TOKENS // ROWS)
    routes = jax.vmap(lambda own, number: assign_block(jax.random.fold_in(streams_of[11], 2), own, number, ROWS, EXPERTS, TOP_K, CAP, 2))(routes_keys, routes_turns).reshape((TOKENS, TOP_K))
    route_weights = jnp.clip(jnp.exp(math.log(2.0) - 2.3025851 * jax.random.uniform(streams_of[12], (TOKENS, TOP_K), jnp.float32) ** levels(streams_of[12], (TOKENS, TOP_K), ((0, 128),), -0.2, 0.2)), 0.2, 2.0)
    expert_gate = gaussian(streams_of[13], (EXPERTS, D, DE), D ** -0.5, 0.125, ((0, 128),))
    expert_up = gaussian(streams_of[14], (EXPERTS, D, DE), D ** -0.5, 0.125, ((0, 128),))
    expert_down = gaussian(streams_of[15], (EXPERTS, DE, D), DE ** -0.5, 0.25, ((0, 128),))
    final_gain = jnp.clip(1.0 + 0.18 * jax.random.normal(streams_of[16], (D,), jnp.float32), 0.1, 1.9)
    final_bias = gaussian(streams_of[17], (D,), 0.3, 1.5, (), jnp.float32)
    return dict(queries=queries, key_heads=key_heads, value_heads=value_heads, documents=documents, query_gain=query_gain, key_gain=key_gain, out_gain=out_gain, out_proj=out_proj, residual=residual, mid_gain=mid_gain, mid_bias=mid_bias, routes=routes, route_weights=route_weights, expert_gate=expert_gate, expert_up=expert_up, expert_down=expert_down, final_gain=final_gain, final_bias=final_bias)


eps_norm = 1e-06
alpha_mix = 8.0 ** 0.25
theta_base = 10000.0

def rotary_tables(row_total, offset):
    positions = offset + jnp.arange(row_total, dtype=jnp.int32)
    grid_row = (positions // GRID).astype(jnp.float32)
    grid_col = (positions % GRID).astype(jnp.float32)
    pair_count = HEAD // 4
    inv_freq = theta_base ** (-jnp.arange(pair_count, dtype=jnp.float32) / pair_count)
    angles = jnp.concatenate([grid_row[:, None] * inv_freq[None, :], grid_col[:, None] * inv_freq[None, :]], axis=1)
    return (jnp.cos(angles), jnp.sin(angles))

def normed_rotated(heads_in, gain_vec, cosine_table, sine_table):
    values = heads_in.astype(jnp.float32)
    inv_rms = lax.rsqrt(lax.optimization_barrier(jnp.mean(values * values, axis=-1, keepdims=True)) + eps_norm)
    values = values * inv_rms * gain_vec
    half_dim = HEAD // 2
    first_half = values[..., :half_dim]
    second_half = values[..., half_dim:]
    cosine_part = cosine_table[:, None, :]
    sine_part = sine_table[:, None, :]
    turned = jnp.concatenate([first_half * cosine_part - second_half * sine_part, second_half * cosine_part + first_half * sine_part], axis=-1)
    return turned.astype(jnp.bfloat16)

def layer_norm(stream, gain_vec, bias_vec):
    center = lax.optimization_barrier(jnp.mean(stream, axis=-1, keepdims=True))
    spread = lax.optimization_barrier(jnp.mean(jnp.square(stream - center), axis=-1, keepdims=True))
    return (stream - center) * lax.rsqrt(spread + eps_norm) * gain_vec + bias_vec

def reference(queries, key_heads, value_heads, documents, query_gain, key_gain, out_gain, out_proj, residual, mid_gain, mid_bias, routes, route_weights, expert_gate, expert_up, expert_down, final_gain, final_bias):
    cosine_table, sine_table = rotary_tables(TOKENS, 0)
    grouped = QH // KVH
    query_rot = normed_rotated(queries.reshape(TOKENS, QH, HEAD), query_gain, cosine_table, sine_table).reshape(TOKENS, KVH, grouped, HEAD)
    key_rot = normed_rotated(key_heads.reshape(TOKENS, KVH, HEAD), key_gain, cosine_table, sine_table).astype(jnp.float32)
    value_all = value_heads.reshape(TOKENS, KVH, HEAD).astype(jnp.float32)
    block_rows = math.gcd(TOKENS, 512)

    def query_block(number):
        first_row = number * block_rows
        query_part = lax.dynamic_slice_in_dim(query_rot, first_row, block_rows, 0).astype(jnp.float32)
        doc_part = lax.dynamic_slice_in_dim(documents, first_row, block_rows, 0)
        scores = jnp.einsum('qkgd,tkd->kgqt', query_part, key_rot) * HEAD ** (-0.5)
        allowed = (doc_part[:, None] == documents[None, :])[None, None]
        scores = jnp.where(allowed, scores, -1e+30)
        row_max = lax.optimization_barrier(jnp.max(scores, axis=-1, keepdims=True))
        weights = jnp.where(allowed, jnp.exp(scores - row_max), 0.0)
        totals = lax.optimization_barrier(jnp.sum(weights, axis=-1))
        rounded = lax.optimization_barrier(weights.astype(jnp.bfloat16)).astype(jnp.float32)
        summed = jnp.einsum('kgqt,tkd->kgqd', rounded, value_all) / totals[..., None]
        return jnp.transpose(summed, (2, 0, 1, 3)).reshape(block_rows, QH * HEAD).astype(jnp.bfloat16)
    attention = lax.map(query_block, jnp.arange(TOKENS // block_rows, dtype=jnp.int32))
    attention = attention.reshape(TOKENS, QH * HEAD)
    attn_float = attention.astype(jnp.float32)
    mean_square = lax.optimization_barrier(jnp.mean(attn_float * attn_float, axis=1, keepdims=True))
    scaled = (attn_float * out_gain).astype(jnp.bfloat16)
    projected = jnp.dot(scaled, out_proj, preferred_element_type=jnp.float32) * lax.rsqrt(mean_square + eps_norm)
    middle = layer_norm(alpha_mix * residual.astype(jnp.float32) + projected, mid_gain, mid_bias).astype(jnp.bfloat16)
    flat_routes = routes.reshape(-1).astype(jnp.int32)
    pair_total = flat_routes.shape[0]
    receive = N_SP * N_TP * CAP
    sorted_order = jnp.argsort(flat_routes, stable=True).astype(jnp.int32)
    counts = lax.optimization_barrier(jnp.sum((flat_routes[:, None] == jnp.arange(EXPERTS, dtype=jnp.int32)[None, :]).astype(jnp.int32), axis=0))
    starts = jnp.cumsum(counts) - counts
    inverse = jnp.zeros((pair_total,), jnp.int32).at[sorted_order].set(jnp.arange(pair_total, dtype=jnp.int32))
    token_of = sorted_order // TOP_K

    def expert_pass(expert):
        slot_index = starts[expert] + jnp.arange(receive, dtype=jnp.int32)
        live_rows = slot_index < starts[expert] + counts[expert]
        source_rows = middle[token_of[jnp.minimum(slot_index, pair_total - 1)]]
        picked = jnp.where(live_rows[:, None], source_rows, jnp.zeros((), jnp.bfloat16))
        gate_part = jnp.dot(picked, expert_gate[expert], preferred_element_type=jnp.float32)
        up_part = jnp.dot(picked, expert_up[expert], preferred_element_type=jnp.float32)
        hidden = (jax.nn.silu(gate_part) * up_part).astype(jnp.bfloat16)
        return jnp.dot(hidden, expert_down[expert], preferred_element_type=jnp.float32).astype(jnp.bfloat16)
    served = lax.map(expert_pass, jnp.arange(EXPERTS, dtype=jnp.int32)).reshape(EXPERTS * receive, D)
    slot_rows = flat_routes * receive + (inverse - starts[flat_routes])
    gathered = served[slot_rows].astype(jnp.float32).reshape(TOKENS, TOP_K, D)
    routed = lax.optimization_barrier(jnp.sum(gathered * route_weights[:, :, None], axis=1))
    return layer_norm(alpha_mix * middle.astype(jnp.float32) + routed, final_gain, final_bias).astype(jnp.bfloat16)
```

```python
import numpy as np

import jax
import jax.numpy as jnp
from jax import lax
from jax.experimental import pallas as pl
from jax.experimental.pallas import tpu as pltpu
from jax.sharding import PartitionSpec as P

HEAD = 128
GRID = 64
TP = 4
SHARE = 4
LANES = 128
TILE = 1024
APART = 32768.0
CAPACITY = 4
PARTS = 4
MARKS = 16

eps_norm = 1e-06
alpha_mix = 8.0**0.25
theta_base = 10000.0
score_scale = HEAD**-0.5 * 1.4426950408889634
f32 = jnp.float32
bf16 = jnp.bfloat16


def angle_tables(row_count):
    pair_count = HEAD // 4
    inv_freq = np.power(
        np.float32(theta_base), -np.arange(pair_count, dtype=np.float32) / np.float32(pair_count)
    ).astype(np.float32)

    def both(count):
        angles = (np.arange(count, dtype=np.float32)[:, None] * inv_freq[None, :]).astype(np.float32)
        return np.cos(angles.astype(np.float64)), np.sin(angles.astype(np.float64))

    row_cos, row_sin = both(row_count)
    col_cos, col_sin = both(GRID)
    none_row, none_col = np.zeros_like(row_cos), np.zeros_like(col_cos)
    row_c = np.concatenate([row_cos, none_row, row_cos, none_row], axis=1)
    row_s = np.concatenate([-row_sin, none_row, row_sin, none_row], axis=1)
    col_c = np.concatenate([none_col, col_cos, none_col, col_cos], axis=1)
    col_s = np.concatenate([none_col, -col_sin, none_col, col_sin], axis=1)
    return np.concatenate([row_c, row_s, col_c, col_s], axis=0).astype(np.float32)


def tables_at(table_ref, first, grid_rows):
    row_count = (table_ref.shape[0] - 2 * GRID) // 2

    def table_of(row_first, col_first):
        row_part = table_ref[pl.ds(pl.multiple_of(row_first, 8), grid_rows)]
        col_part = table_ref[col_first : col_first + GRID]
        return (row_part[:, None, :] + col_part[None, :, :]).reshape(grid_rows * GRID, HEAD)

    return (
        table_of(first, 2 * row_count),
        table_of(row_count + first, 2 * row_count + GRID),
    )


def normed_rotated(values, gain_row, cosine, sine):
    inv_rms = lax.rsqrt(jnp.mean(values * values, axis=-1, keepdims=True) + eps_norm)
    values = values * inv_rms * gain_row
    return (values * cosine + pltpu.roll(values, HEAD // 2, 1) * sine).astype(bf16)


def key_kernel(
    index_ref, key_hbm, value_hbm, doc_hbm, gain_hbm, table_hbm, out_hbm,
    key_ref, value_ref, doc_ref, gain_ref, table_ref, built_ref, in_sems, out_sems,
):
    pairs = (
        (key_hbm, key_ref), (value_hbm, value_ref), (doc_hbm, doc_ref), (gain_hbm, gain_ref),
        (table_hbm, table_ref),
    )
    arriving = [pltpu.make_async_copy(a, b, in_sems.at[i]) for i, (a, b) in enumerate(pairs)]
    for copy in arriving:
        copy.start()
    for copy in arriving:
        copy.wait()
    tok_rows = key_ref.shape[0]
    grid_rows = tok_rows // GRID
    cosine, sine = tables_at(table_ref, index_ref[0] * grid_rows, grid_rows)
    rotated = normed_rotated(key_ref[...].astype(f32), gain_ref[...], cosine, sine)
    numbers = lax.broadcasted_iota(jnp.int32, (MARKS, tok_rows), 0)
    documents = doc_ref[...]
    marks = jnp.where(numbers == documents, 1.0, 0.0)
    marks = jnp.where(numbers == MARKS - 1, documents.astype(f32), marks).astype(bf16)
    built_ref[:HEAD, :] = jnp.transpose(rotated.astype(f32)).astype(bf16)
    built_ref[HEAD : HEAD + MARKS, :] = marks
    for g in range(tok_rows // HEAD):
        built_ref[HEAD + MARKS :, g * HEAD : (g + 1) * HEAD] = value_ref[
            g * HEAD : (g + 1) * HEAD, :
        ]
    leaving = [
        pltpu.make_async_copy(built_ref, out_hbm.at[i], out_sems.at[i])
        for i in range(out_hbm.shape[0])
    ]
    for copy in leaving:
        copy.start()
    for copy in leaving:
        copy.wait()


def query_kernel(index_ref, *refs):
    query_refs = refs[:SHARE]
    gain_ref, table_ref, out_hbm, out_ref, out_sems = refs[SHARE:]
    tok_rows = query_refs[0].shape[0] - MARKS
    width = query_refs[0].shape[1]
    grid_rows = tok_rows // GRID
    own = index_ref[0] % SHARE
    numbers = lax.broadcasted_iota(jnp.int32, (LANES, tok_rows), 0).astype(f32)
    for i, query_ref in enumerate(query_refs):
        place = own ^ i
        cosine, sine = tables_at(
            table_ref, (index_ref[0] - own + place) * grid_rows, grid_rows
        )
        lines = query_ref[tok_rows:, :].astype(f32)
        documents = jnp.concatenate([lines[k : k + 1] for k in range(tok_rows // width)], axis=1)
        apart = jnp.where(numbers == documents, 0.0, -APART)
        apart = jnp.where(numbers >= MARKS - 2, 0.0, apart)
        apart = jnp.where(numbers == MARKS - 2, documents, apart)
        apart = jnp.transpose(apart).astype(bf16)
        rows = pl.ds(pl.multiple_of(place * tok_rows, tok_rows), tok_rows)
        for h in range(out_ref.shape[0]):
            values = query_ref[:tok_rows, h * HEAD : (h + 1) * HEAD].astype(f32)
            out_ref[h, rows, :HEAD] = normed_rotated(values, gain_ref[...], cosine, sine)
            out_ref[h, rows, HEAD:] = apart
    leaving = [
        pltpu.make_async_copy(out_ref.at[h], out_hbm.at[h], out_sems.at[h])
        for h in range(out_ref.shape[0])
    ]
    for copy in leaving:
        copy.start()
    for copy in leaving:
        copy.wait()


def attention_kernel(
    small_ref, query_hbm, kv_ref, out_ref, keys_ref, first_ref, last_ref, acc_ref, total_ref,
    max_ref, tiles_ref, sems,
):
    heads, _, depth = query_hbm.shape
    shards, _, tok_rows = kv_ref.shape
    rows = acc_ref.shape[0]
    tile = rows // heads
    marked = HEAD + MARKS
    step = pl.program_id(0)
    steps = query_hbm.shape[1] // tile
    arriving = [
        pltpu.make_async_copy(
            query_hbm.at[:, pl.ds(i * tile, tile), :], tiles_ref.at[i], sems.at[i]
        )
        for i in range(steps)
    ]

    @pl.when(step == 0)
    def fetch():
        for copy in arriving:
            copy.start()


    @pl.when(step == 0)
    def fill():
        for j in range(shards):
            keys_ref[j, :marked, :] = kv_ref[j, :marked, :]
            keys_ref[j, marked:, :] = jnp.zeros((depth - marked, tok_rows), bf16)
            line = kv_ref[j, HEAD:marked, :].astype(f32)
            first_ref[j] = line[MARKS - 1, 0].astype(jnp.int32)
            last_ref[j] = line[MARKS - 1, tok_rows - 1].astype(jnp.int32)

    for i in range(steps):
        pl.when(step == i)(arriving[i].wait)
    query_ref = tiles_ref.at[step]
    queries = query_ref[...].reshape(rows, depth)
    top = query_ref[0, :16, HEAD:].astype(f32)
    bottom = query_ref[0, tile - 16 :, HEAD:].astype(f32)
    low = top[0, MARKS - 2].astype(jnp.int32)
    high = bottom[15, MARKS - 2].astype(jnp.int32)
    from_shard = jnp.int32(0)
    to_shard = jnp.int32(0)
    for j in range(shards):
        from_shard += (last_ref[j] < low).astype(jnp.int32)
        to_shard += (first_ref[j] <= high).astype(jnp.int32)

    acc_ref[...] = jnp.zeros_like(acc_ref)
    total_ref[...] = jnp.zeros_like(total_ref)

    def scores_of(j):
        return jnp.dot(queries, keys_ref[j], preferred_element_type=f32)

    def values_of(j):
        return jnp.concatenate(
            [kv_ref[j, marked:, g * HEAD : (g + 1) * HEAD] for g in range(tok_rows // HEAD)],
            axis=0,
        )

    def folded(weights):
        part = weights[:, :LANES]
        for i in range(1, weights.shape[1] // LANES):
            part = part + weights[:, i * LANES : (i + 1) * LANES]
        return part

    @pl.when(small_ref[0] == 1)
    def without_max():
        max_ref[...] = jnp.zeros_like(max_ref)

        def advance(j, unused):
            weights = jnp.exp2(scores_of(j) * score_scale)
            total_ref[...] += folded(weights)
            acc_ref[...] += jnp.dot(
                weights.astype(bf16), values_of(j), preferred_element_type=f32
            )
            return unused

        lax.fori_loop(from_shard, to_shard, advance, 0)

    @pl.when(small_ref[0] == 0)
    def with_max():
        max_ref[...] = jnp.full_like(max_ref, -1e30)

        def advance(j, unused):
            scores = scores_of(j) * score_scale
            old_max = max_ref[...]
            new_max = jnp.maximum(old_max, jnp.max(scores, axis=1, keepdims=True))
            weights = jnp.exp2(scores - new_max[:, :1])
            rescale = jnp.exp2(old_max - new_max)
            max_ref[...] = new_max
            total_ref[...] = total_ref[...] * rescale + folded(weights)
            acc_ref[...] = acc_ref[...] * rescale + jnp.dot(
                weights.astype(bf16), values_of(j), preferred_element_type=f32
            )
            return unused

        lax.fori_loop(from_shard, to_shard, advance, 0)

    rows_out = LANES
    eye = lax.broadcasted_iota(jnp.int32, (rows_out, LANES), 0) == lax.broadcasted_iota(
        jnp.int32, (rows_out, LANES), 1
    )
    for h in range(heads):
        for i in range(tile // rows_out):
            mine = slice(h * tile + i * rows_out, h * tile + (i + 1) * rows_out)
            lanes = slice(h * HEAD, (h + 1) * HEAD)
            total = jnp.sum(total_ref[mine], axis=1, keepdims=True)
            some = total > 0.0
            held = jnp.where(some, total, 1.0)
            out_ref[i, :rows_out, lanes] = (acc_ref[mine] / held).astype(bf16)
            level = jnp.where(some, max_ref[mine] + jnp.log2(held), -1e30)
            flat = jnp.sum(jnp.where(eye, level, 0.0), axis=0, keepdims=True)
            top = flat.astype(bf16).astype(f32)
            rest = flat - top
            middle = rest.astype(bf16).astype(f32)
            final = rest - middle
            out_ref[i, rows_out:, lanes] = jnp.concatenate(
                [top, middle, final, jnp.zeros((13, LANES), f32)], axis=0
            ).astype(bf16)


def layer_norm(stream, gain_row, bias_row):
    center = jnp.mean(stream, axis=-1, keepdims=True)
    spread = jnp.mean(jnp.square(stream - center), axis=-1, keepdims=True)
    return (stream - center) * lax.rsqrt(spread + eps_norm) * gain_row + bias_row


def middle_kernel(
    part_ref, out_gain_ref, proj_ref, residual_ref, gain_ref, bias_ref, target_ref,
    middle_ref, outbound_ref, held_ref, sem_ref,
):
    sources, _, width = part_ref.shape
    copies = [
        pltpu.make_async_copy(
            proj_ref.at[pl.ds(t * width, width)], held_ref.at[pl.ds(t * width, width)], sem_ref.at[t]
        )
        for t in range(TP)
    ]
    for copy in copies:
        copy.start()
    rows = LANES
    heads = width // HEAD
    levels = jnp.sum(part_ref[:, rows:, :].astype(f32), axis=1)
    pieces = [levels[i * TP : (i + 1) * TP] for i in range(SHARE)]
    highest = pieces[0]
    for piece in pieces[1:]:
        highest = jnp.maximum(highest, piece)
    shares = [jnp.exp2(piece - highest) for piece in pieces]
    whole = shares[0]
    for share in shares[1:]:
        whole = whole + share
    shares = jnp.concatenate([share / whole for share in shares], axis=0)
    columns = []
    for h in range(heads):
        square = jnp.concatenate(
            [
                shares[:, h * HEAD : (h + 1) * HEAD],
                jnp.zeros((LANES - sources, LANES), f32),
            ],
            axis=0,
        )
        columns.append(jnp.transpose(square))
    attended = []
    for t in range(TP):
        for h in range(heads):
            mixed = jnp.zeros((rows, HEAD), f32)
            for i in range(SHARE):
                source = i * TP + t
                mixed = mixed + columns[h][:, source : source + 1] * part_ref[
                    source, :rows, h * HEAD : (h + 1) * HEAD
                ].astype(f32)
            attended.append(mixed.astype(bf16).astype(f32))
    attention = jnp.concatenate(attended, axis=1)
    mean_square = jnp.mean(attention * attention, axis=1, keepdims=True)
    scaled = (attention * out_gain_ref[...]).astype(bf16)
    projected = jnp.zeros((rows, held_ref.shape[1]), f32)
    for t in range(TP):
        copies[t].wait()
        lanes = slice(t * width, (t + 1) * width)
        projected = projected + jnp.dot(
            scaled[:, lanes], held_ref[lanes, :], preferred_element_type=f32
        )
    projected = projected * lax.rsqrt(mean_square + eps_norm)
    middle = layer_norm(
        alpha_mix * residual_ref[...].astype(f32) + projected, gain_ref[...], bias_ref[...]
    ).astype(bf16)
    middle_ref[...] = middle
    cut = middle.shape[1] // PARTS
    stacked = jnp.concatenate([middle[:, p * cut : (p + 1) * cut] for p in range(PARTS)], axis=0)
    out_rows = outbound_ref.shape[0]
    count = 4
    some = out_rows // count
    for c in range(count):
        row = c * some + lax.broadcasted_iota(jnp.int32, (some, PARTS * rows), 0)
        part = (row // CAPACITY) % PARTS
        slot = (row // (CAPACITY * PARTS)) * CAPACITY + row % CAPACITY
        lane = lax.broadcasted_iota(jnp.int32, (some, PARTS * rows), 1)
        code = jnp.where(part == lane // rows, slot, -1)
        chosen = (code == target_ref[0:1, :]) | (code == target_ref[1:2, :])
        outbound_ref[c * some : (c + 1) * some, :] = jnp.dot(
            jnp.where(chosen, 1.0, 0.0).astype(bf16), stacked, preferred_element_type=f32
        ).astype(bf16)


def swap_matrix(size):
    group = CAPACITY * PARTS
    tiles = size // group
    row = lax.broadcasted_iota(jnp.int32, (size, size), 0)
    col = lax.broadcasted_iota(jnp.int32, (size, size), 1)
    part = row // (tiles * CAPACITY)
    tile = (row // CAPACITY) % tiles
    inner = row % CAPACITY
    return jnp.where(col == tile * group + part * CAPACITY + inner, 1.0, 0.0).astype(bf16)


def expert_kernel(arrived_ref, gate_ref, up_ref, down_ref, served_ref, rows_ref, swap_ref):
    chunk = 256
    chunks = arrived_ref.shape[0] // chunk
    cut = arrived_ref.shape[1]
    some = chunk // PARTS
    swap_ref[...] = swap_matrix(chunk)
    for c in range(chunks):
        sorted_rows = jnp.dot(
            swap_ref[...], arrived_ref[c * chunk : (c + 1) * chunk, :], preferred_element_type=f32
        ).astype(bf16)
        for p in range(PARTS):
            rows_ref[c * some : (c + 1) * some, p * cut : (p + 1) * cut] = sorted_rows[
                p * some : (p + 1) * some
            ]
    rows = rows_ref[...]
    gate = jnp.dot(rows, gate_ref[...], preferred_element_type=f32)
    up = jnp.dot(rows, up_ref[...], preferred_element_type=f32)
    hidden = (gate / (1.0 + jnp.exp(-gate)) * up).astype(bf16)
    rows_ref[...] = jnp.dot(hidden, down_ref[...], preferred_element_type=f32).astype(bf16)
    for c in range(chunks):
        stacked = jnp.concatenate(
            [
                rows_ref[c * some : (c + 1) * some, p * cut : (p + 1) * cut]
                for p in range(PARTS)
            ],
            axis=0,
        )
        served_ref[c * chunk : (c + 1) * chunk, :] = lax.dot_general(
            swap_ref[...], stacked, (((0,), (0,)), ((), ())), preferred_element_type=f32
        ).astype(bf16)


def final_kernel(
    returned_ref, target_ref, weight_ref, middle_ref, gain_ref, bias_ref, out_ref, routed_ref
):
    rows = middle_ref.shape[0]
    all_rows, cut = returned_ref.shape
    col = lax.broadcasted_iota(jnp.int32, (rows, all_rows), 1)
    part = (col // CAPACITY) % PARTS
    slot = (col // (CAPACITY * PARTS)) * CAPACITY + col % CAPACITY
    for k in range(2):
        hit = slot == target_ref[:, k : k + 1]
        weight = weight_ref[:, k : k + 1]
        for p in range(PARTS):
            chosen = jnp.where(hit & (part == p), 1.0, 0.0).astype(bf16)
            picked = jnp.dot(chosen, returned_ref[...], preferred_element_type=f32) * weight
            lanes = slice(p * cut, (p + 1) * cut)
            routed_ref[:, lanes] = picked if k == 0 else routed_ref[:, lanes] + picked
    out_ref[...] = layer_norm(
        alpha_mix * middle_ref[...].astype(f32) + routed_ref[...], gain_ref[...], bias_ref[...]
    ).astype(bf16)


def whole_vmem():
    return pl.BlockSpec(memory_space=pltpu.VMEM)


def in_hbm():
    return pl.BlockSpec(memory_space=pltpu.HBM)


def held(array):
    return pltpu.with_memory_space_constraint(array, pltpu.HBM)


def in_smem():
    return pl.BlockSpec(memory_space=pltpu.SMEM)


def params(mib, grid=0):
    more = {"dimension_semantics": ("arbitrary",)} if grid else {}
    return pltpu.CompilerParams(vmem_limit_bytes=mib << 20, **more)


def attention_call(small, shared_rot, kv_all):
    heads, all_rows, depth = shared_rot.shape
    shards, _, tok_rows = kv_all.shape
    tile = TILE
    width = heads * HEAD
    return pl.pallas_call(
        attention_kernel,
        grid=(all_rows // tile,),
        out_shape=jax.ShapeDtypeStruct((all_rows // LANES, LANES + 16, width), bf16),
        in_specs=[
            in_smem(),
            in_hbm(),
            whole_vmem(),
        ],
        out_specs=pl.BlockSpec((tile // LANES, LANES + 16, width), lambda i: (i, 0, 0)),
        scratch_shapes=[
            pltpu.VMEM((shards, depth, tok_rows), bf16),
            pltpu.SMEM((shards,), jnp.int32),
            pltpu.SMEM((shards,), jnp.int32),
            pltpu.VMEM((heads * tile, HEAD), f32),
            pltpu.VMEM((heads * tile, HEAD), f32),
            pltpu.VMEM((heads * tile, HEAD), f32),
            pltpu.VMEM((all_rows // tile, heads, tile, depth), bf16),
            pltpu.SemaphoreType.DMA((all_rows // tile,)),
        ],
        compiler_params=params(40, 1),
        name="document_attention",
    )(small, held(shared_rot), kv_all)


def per_device(
    queries, key_heads, value_heads, documents, query_gain, key_gain, out_gain, out_proj,
    residual, mid_gain, mid_bias, routes, route_weights, expert_gate, expert_up, expert_down,
    final_gain, final_bias,
):
    tok_rows, width = queries.shape
    heads = width // HEAD
    sp_size = lax.axis_size("sp")
    tp_size = lax.axis_size("tp")
    shards = sp_size // SHARE
    table = jnp.asarray(angle_tables(sp_size * tok_rows // GRID))
    index = lax.axis_index("sp").astype(jnp.int32).reshape(1)
    class_groups = [[c + SHARE * j for j in range(shards)] for c in range(SHARE)]
    owner_groups = [
        [(g * SHARE + i) * tp_size + t for i in range(SHARE) for t in range(tp_size)]
        for g in range(shards)
    ]

    kv_rows = 2 * HEAD + MARKS
    kv = pl.pallas_call(
        key_kernel,
        out_shape=pltpu.HBM((shards, kv_rows, tok_rows), bf16),
        in_specs=[in_smem()] + [in_hbm()] * 5,
        out_specs=in_hbm(),
        scratch_shapes=[
            pltpu.VMEM(key_heads.shape, bf16),
            pltpu.VMEM(value_heads.shape, bf16),
            pltpu.VMEM((1, tok_rows), jnp.int32),
            pltpu.VMEM((1, HEAD), f32),
            pltpu.VMEM(table.shape, f32),
            pltpu.VMEM((kv_rows, tok_rows), bf16),
            pltpu.SemaphoreType.DMA((5,)),
            pltpu.SemaphoreType.DMA((shards,)),
        ],
        compiler_params=params(16),
        name="key_rotation",
    )(
        index, held(key_heads), held(value_heads), held(documents.reshape(1, tok_rows)),
        held(key_gain.reshape(1, HEAD)), held(table),
    )
    kv_all = lax.all_to_all(kv, "sp", 0, 0, tiled=True, axis_index_groups=class_groups)

    lines = documents.astype(bf16).reshape(tok_rows // width, width)
    marked = jnp.concatenate(
        [queries, lines, jnp.zeros((MARKS - tok_rows // width, width), bf16)], axis=0
    )
    shared = [marked]
    for k in range(1, SHARE):
        shared.append(lax.ppermute(marked, "sp", [(i, i ^ k) for i in range(sp_size)]))

    shared_rot = pl.pallas_call(
        query_kernel,
        out_shape=pltpu.HBM((heads, SHARE * tok_rows, 2 * HEAD), bf16),
        in_specs=[in_smem()] + [whole_vmem()] * (SHARE + 2),
        out_specs=in_hbm(),
        scratch_shapes=[
            pltpu.VMEM((heads, SHARE * tok_rows, 2 * HEAD), bf16),
            pltpu.SemaphoreType.DMA((heads,)),
        ],
        compiler_params=params(24),
        name="query_rotation",
    )(index, *shared, query_gain.reshape(1, HEAD), table)

    largest = jnp.max(jnp.abs(query_gain)) * jnp.max(jnp.abs(key_gain))
    small = (largest * (HEAD * score_scale * 1.02) < 50.0).astype(jnp.int32).reshape(1)
    partial = attention_call(small, shared_rot, kv_all)
    partial = lax.all_to_all(
        partial, ("sp", "tp"), 0, 0, tiled=True, axis_index_groups=owner_groups
    )

    out_rows, model_width = residual.shape
    expert_total = sp_size * tp_size
    flat = routes.T.reshape(-1)
    order = jnp.arange(flat.shape[0], dtype=jnp.int32)
    earlier = (flat[:, None] == flat[None, :]) & (order[None, :] < order[:, None])
    rank = jnp.sum(earlier.astype(jnp.int32), axis=1)
    target = (flat * CAPACITY + rank).reshape(2, out_rows)

    cut = model_width // PARTS
    exchange_rows = expert_total * CAPACITY * PARTS
    middle, outbound = pl.pallas_call(
        middle_kernel,
        out_shape=(
            jax.ShapeDtypeStruct((out_rows, model_width), bf16),
            jax.ShapeDtypeStruct((exchange_rows, cut), bf16),
        ),
        in_specs=[
            whole_vmem(), whole_vmem(), in_hbm(), whole_vmem(),
            whole_vmem(), whole_vmem(), whole_vmem(),
        ],
        out_specs=(whole_vmem(), whole_vmem()),
        scratch_shapes=[
            pltpu.VMEM(out_proj.shape, bf16),
            pltpu.SemaphoreType.DMA((TP,)),
        ],
        compiler_params=params(40),
        name="middle_stream",
    )(
        partial, out_gain.reshape(1, -1), held(out_proj), residual, mid_gain.reshape(1, -1),
        mid_bias.reshape(1, -1), jnp.tile(target, (1, PARTS)),
    )
    arrived = lax.all_to_all(
        outbound.reshape(expert_total, CAPACITY * PARTS, cut), ("sp", "tp"), 0, 0, tiled=True
    )
    hidden_width = expert_gate.shape[2]
    served = pl.pallas_call(
        expert_kernel,
        out_shape=jax.ShapeDtypeStruct((exchange_rows, cut), bf16),
        in_specs=[whole_vmem() for _ in range(4)],
        out_specs=whole_vmem(),
        scratch_shapes=[
            pltpu.VMEM((expert_total * CAPACITY, model_width), bf16),
            pltpu.VMEM((256, 256), bf16),
        ],
        compiler_params=params(40),
        name="expert",
    )(
        arrived.reshape(exchange_rows, cut),
        expert_gate.reshape(model_width, hidden_width),
        expert_up.reshape(model_width, hidden_width),
        expert_down.reshape(hidden_width, model_width),
    )
    returned = lax.all_to_all(
        served.reshape(expert_total, CAPACITY * PARTS, cut), ("sp", "tp"), 0, 0, tiled=True
    )
    return pl.pallas_call(
        final_kernel,
        out_shape=jax.ShapeDtypeStruct((out_rows, model_width), bf16),
        in_specs=[whole_vmem() for _ in range(6)],
        out_specs=whole_vmem(),
        scratch_shapes=[pltpu.VMEM((out_rows, model_width), f32)],
        compiler_params=params(40),
        name="final_stream",
    )(
        returned.reshape(exchange_rows, cut), target.T, route_weights, middle,
        final_gain.reshape(1, -1), final_bias.reshape(1, -1),
    )


def solution(mesh):
    rows = P(("sp", "tp"), None)
    experts = P(("sp", "tp"), None, None)
    return jax.shard_map(
        per_device,
        mesh=mesh,
        in_specs=(
            P("sp", "tp"), P("sp", "tp"), P("sp", "tp"), P("sp"), P(), P(), P(), P(), rows, P(),
            P(), rows, rows, experts, experts, experts, P(), P(),
        ),
        out_specs=rows,
        check_vma=False,
    )
```

```python
import numpy as np

import jax
import jax.numpy as jnp
from jax import lax
from jax.experimental import pallas as pl
from jax.experimental.pallas import tpu as pltpu
from jax.sharding import PartitionSpec as P

HEAD = 128
GRID = 64
TP = 4
SHARE = 4
LANES = 128
TILE = 2048
APART = 32768.0
CAPACITY = 4
PARTS = 4
SHARDS = 8
MARKS = 16

eps_norm = 1e-06
alpha_mix = 8.0**0.25
theta_base = 10000.0
score_scale = HEAD**-0.5 * 1.4426950408889634
f32 = jnp.float32
bf16 = jnp.bfloat16


def angle_tables(row_count):
    pair_count = HEAD // 4
    inv_freq = np.power(
        np.float32(theta_base), -np.arange(pair_count, dtype=np.float32) / np.float32(pair_count)
    ).astype(np.float32)

    def both(count):
        angles = (np.arange(count, dtype=np.float32)[:, None] * inv_freq[None, :]).astype(np.float32)
        return np.cos(angles.astype(np.float64)), np.sin(angles.astype(np.float64))

    row_cos, row_sin = both(row_count)
    col_cos, col_sin = both(GRID)
    none_row, none_col = np.zeros_like(row_cos), np.zeros_like(col_cos)
    row_c = np.concatenate([row_cos, none_row, row_cos, none_row], axis=1)
    row_s = np.concatenate([-row_sin, none_row, row_sin, none_row], axis=1)
    col_c = np.concatenate([none_col, col_cos, none_col, col_cos], axis=1)
    col_s = np.concatenate([none_col, -col_sin, none_col, col_sin], axis=1)
    return np.concatenate([row_c, row_s, col_c, col_s], axis=0).astype(np.float32)


def tables_at(table_ref, first, grid_rows):
    row_count = (table_ref.shape[0] - 2 * GRID) // 2

    def table_of(row_first, col_first):
        row_part = table_ref[pl.ds(pl.multiple_of(row_first, 8), grid_rows)]
        col_part = table_ref[col_first : col_first + GRID]
        return (row_part[:, None, :] + col_part[None, :, :]).reshape(grid_rows * GRID, HEAD)

    return (
        table_of(first, 2 * row_count),
        table_of(row_count + first, 2 * row_count + GRID),
    )


def normed_rotated(values, gain_row, cosine, sine):
    inv_rms = lax.rsqrt(jnp.mean(values * values, axis=-1, keepdims=True) + eps_norm)
    values = values * inv_rms * gain_row
    return (values * cosine + pltpu.roll(values, HEAD // 2, 1) * sine).astype(bf16)


def key_kernel(
    index_ref, key_hbm, value_hbm, doc_hbm, gain_hbm, table_hbm, query_hbm, out_hbm, marked_hbm,
    key_ref, value_ref, doc_ref, gain_ref, table_ref, built_ref, lines_ref, in_sems, out_sems,
):
    tok_rows, width = query_hbm.shape
    passing = pltpu.make_async_copy(query_hbm, lines_ref.at[pl.ds(0, tok_rows)], in_sems.at[5])
    pairs = (
        (key_hbm, key_ref), (value_hbm, value_ref), (doc_hbm, doc_ref), (gain_hbm, gain_ref),
        (table_hbm, table_ref),
    )
    arriving = [pltpu.make_async_copy(a, b, in_sems.at[i]) for i, (a, b) in enumerate(pairs)]
    for copy in arriving:
        copy.start()
    passing.start()
    for copy in arriving:
        copy.wait()
    grid_rows = tok_rows // GRID
    cosine, sine = tables_at(table_ref, index_ref[0] * grid_rows, grid_rows)
    rotated = normed_rotated(key_ref[...].astype(f32), gain_ref[...], cosine, sine)
    numbers = lax.broadcasted_iota(jnp.int32, (MARKS, tok_rows), 0)
    documents = doc_ref[...]
    marks = jnp.where(numbers == documents, 1.0, 0.0)
    marks = jnp.where(numbers == MARKS - 1, documents.astype(f32), marks).astype(bf16)
    built_ref[:HEAD, :] = jnp.transpose(rotated.astype(f32)).astype(bf16)
    built_ref[HEAD : HEAD + MARKS, :] = marks
    for g in range(tok_rows // HEAD):
        built_ref[HEAD + MARKS :, g * HEAD : (g + 1) * HEAD] = value_ref[
            g * HEAD : (g + 1) * HEAD, :
        ]
    leaving = pltpu.make_async_copy(built_ref, out_hbm, out_sems.at[0])
    leaving.start()
    lines = [
        documents[:, i * width : (i + 1) * width].astype(f32) for i in range(tok_rows // width)
    ]
    lines.append(jnp.zeros((MARKS - len(lines), width), f32))
    lines_ref[tok_rows:, :] = jnp.concatenate(lines, axis=0).astype(bf16)
    passing.wait()
    marking = pltpu.make_async_copy(lines_ref, marked_hbm, out_sems.at[1])
    marking.start()
    leaving.wait()
    marking.wait()


def query_kernel(index_ref, *refs):
    query_hbms = refs[:SHARE]
    (
        gain_hbm, table_hbm, out_hbm, out_ref, gain_ref, table_ref, query_refs, out_sems, in_sems,
    ) = refs[SHARE:]
    arriving = [
        pltpu.make_async_copy(query_hbm, query_refs.at[i], in_sems.at[2 + i])
        for i, query_hbm in enumerate(query_hbms)
    ] + [
        pltpu.make_async_copy(gain_hbm, gain_ref, in_sems.at[0]),
        pltpu.make_async_copy(table_hbm, table_ref, in_sems.at[1]),
    ]
    for copy in arriving:
        copy.start()
    for copy in arriving:
        copy.wait()
    tok_rows = query_refs.shape[1] - MARKS
    width = query_refs.shape[2]
    grid_rows = tok_rows // GRID
    own = index_ref[0] % SHARE
    numbers = lax.broadcasted_iota(jnp.int32, (LANES, tok_rows), 0).astype(f32)
    for i in range(SHARE):
        query_ref = query_refs.at[i]
        place = own ^ i
        cosine, sine = tables_at(
            table_ref, (index_ref[0] - own + place) * grid_rows, grid_rows
        )
        lines = query_ref[tok_rows:, :].astype(f32)
        documents = jnp.concatenate([lines[k : k + 1] for k in range(tok_rows // width)], axis=1)
        apart = jnp.where(numbers == documents, 0.0, -APART)
        apart = jnp.where(numbers >= MARKS - 2, 0.0, apart)
        apart = jnp.where(numbers == MARKS - 2, documents, apart)
        apart = jnp.transpose(apart).astype(bf16)
        half = 0 if i % 2 else SHARE // 2
        rows = pl.ds(pl.multiple_of((half + place // 2) * tok_rows, tok_rows), tok_rows)
        for h in range(out_ref.shape[0]):
            values = query_ref[:tok_rows, h * HEAD : (h + 1) * HEAD].astype(f32)
            out_ref[h, rows, :HEAD] = normed_rotated(values, gain_ref[...], cosine, sine)
            out_ref[h, rows, HEAD:] = apart
    leaving = [
        pltpu.make_async_copy(out_ref.at[h], out_hbm.at[h], out_sems.at[h])
        for h in range(out_ref.shape[0])
    ]
    for copy in leaving:
        copy.start()
    for copy in leaving:
        copy.wait()


def attention_kernel(query_gain_ref, key_gain_ref, query_hbm, *refs):
    kv_refs = refs[:SHARDS]
    refs = refs[SHARDS:]
    (
        out_ref, keys_ref, values_ref, first_ref, last_ref, order_ref, small_ref, acc_ref, total_ref, max_ref,
        tiles_ref, tile_sems, key_sems, value_sems,
    ) = refs
    heads, all_rows, depth = query_hbm.shape
    tok_rows = keys_ref.shape[2]
    rows = acc_ref.shape[0]
    tile = rows // heads
    marked = HEAD + MARKS
    groups = tok_rows // HEAD
    step = pl.program_id(0)
    steps = all_rows // tile
    tiles = [
        pltpu.make_async_copy(
            query_hbm.at[:, pl.ds(i * tile, tile), :], tiles_ref.at[i], tile_sems.at[i]
        )
        for i in range(steps)
    ]

    @pl.when(step == 0)
    def fetch():
        arriving = []
        for j, kv_ref in enumerate(kv_refs):
            arriving.append(
                pltpu.make_async_copy(
                    kv_ref.at[pl.ds(0, marked)], keys_ref.at[j, pl.ds(0, marked)], key_sems.at[j]
                )
            )
        tiles_first = tiles[:1]
        for j, kv_ref in enumerate(kv_refs):
            for g in range(groups):
                arriving.append(
                    pltpu.make_async_copy(
                        kv_ref.at[pl.ds(marked, HEAD), pl.ds(g * HEAD, HEAD)],
                        values_ref.at[j, pl.ds(g * HEAD, HEAD)],
                        value_sems.at[j * groups + g],
                    )
                )
        for copy in tiles_first + arriving + tiles[1:]:
            copy.start()
        largest = jnp.max(jnp.abs(query_gain_ref[...])) * jnp.max(jnp.abs(key_gain_ref[...]))
        small_ref[0] = (largest * (HEAD * score_scale * 1.02) < 50.0).astype(jnp.int32)
        for j in range(SHARDS):
            keys_ref[j, marked:, :] = jnp.zeros((depth - marked, tok_rows), bf16)
        for copy in arriving:
            copy.wait()
        for j in range(SHARDS):
            line = keys_ref[j, HEAD:marked, :].astype(f32)
            first_ref[j] = line[MARKS - 1, 0].astype(jnp.int32)
            last_ref[j] = line[MARKS - 1, tok_rows - 1].astype(jnp.int32)

    for i in range(steps):
        pl.when(step == i)(tiles[i].wait)
    query_ref = tiles_ref.at[step]
    queries = query_ref[...].reshape(rows, depth)
    low = jnp.int32(1 << 20)
    high = jnp.int32(-1)
    half = all_rows // 2
    for begin in range(0, tile, half):
        top = query_ref[0, begin : begin + 16, HEAD:].astype(f32)
        bottom = query_ref[0, begin + half - 16 : begin + half, HEAD:].astype(f32)
        low = jnp.minimum(low, top[0, MARKS - 2].astype(jnp.int32))
        high = jnp.maximum(high, bottom[15, MARKS - 2].astype(jnp.int32))
    count = jnp.int32(0)
    for j in range(SHARDS):
        order_ref[count] = jnp.int32(j)
        count += ((first_ref[j] <= high) & (last_ref[j] >= low)).astype(jnp.int32)

    acc_ref[...] = jnp.zeros_like(acc_ref)
    total_ref[...] = jnp.zeros_like(total_ref)

    def scores_of(j):
        return jnp.dot(queries, keys_ref[j], preferred_element_type=f32)

    def folded(weights):
        part = weights[:, :LANES]
        for i in range(1, weights.shape[1] // LANES):
            part = part + weights[:, i * LANES : (i + 1) * LANES]
        return part

    @pl.when(small_ref[0] == 1)
    def without_max():
        max_ref[...] = jnp.zeros_like(max_ref)

        def advance(i, unused):
            j = order_ref[i]
            weights = jnp.exp2(scores_of(j) * score_scale)
            total_ref[...] += folded(weights)
            acc_ref[...] += jnp.dot(
                weights.astype(bf16), values_ref[j], preferred_element_type=f32
            )
            return unused

        lax.fori_loop(0, count, advance, 0)

    @pl.when(small_ref[0] == 0)
    def with_max():
        max_ref[...] = jnp.full_like(max_ref, -1e30)

        some_rows = 512

        def advance(i, unused):
            j = order_ref[i]

            def some_of(r, unused):
                mine = pl.ds(pl.multiple_of((r % (tile // some_rows)) * some_rows, some_rows), some_rows)
                held = pl.ds(pl.multiple_of(r * some_rows, some_rows), some_rows)
                part = query_ref[r // (tile // some_rows), mine, :]
                scores = jnp.dot(part, keys_ref[j], preferred_element_type=f32) * score_scale
                old_max = max_ref[held]
                new_max = jnp.maximum(old_max, jnp.max(scores, axis=1, keepdims=True))
                weights = jnp.exp2(scores - new_max[:, :1])
                rescale = jnp.exp2(old_max - new_max)
                max_ref[held] = new_max
                total_ref[held] = total_ref[held] * rescale + folded(weights)
                acc_ref[held] = acc_ref[held] * rescale + jnp.dot(
                    weights.astype(bf16), values_ref[j], preferred_element_type=f32
                )
                return unused

            return lax.fori_loop(0, rows // some_rows, some_of, unused)

        lax.fori_loop(0, count, advance, 0)

    rows_out = LANES
    eye = lax.broadcasted_iota(jnp.int32, (rows_out, LANES), 0) == lax.broadcasted_iota(
        jnp.int32, (rows_out, LANES), 1
    )
    for h in range(heads):
        for i in range(tile // rows_out):
            mine = slice(h * tile + i * rows_out, h * tile + (i + 1) * rows_out)
            lanes = slice(h * HEAD, (h + 1) * HEAD)
            total = jnp.sum(total_ref[mine], axis=1, keepdims=True)
            some = total > 0.0
            kept = jnp.where(some, total, 1.0)
            level = jnp.where(some, max_ref[mine] + jnp.log2(kept), -1e30)
            share = 1.0 / kept
            mixed = acc_ref[mine] * share
            out_ref[i, :rows_out, lanes] = mixed.astype(bf16)
            flat = jnp.sum(jnp.where(eye, level, 0.0), axis=0, keepdims=True)
            top = flat.astype(bf16).astype(f32)
            rest = flat - top
            middle = rest.astype(bf16).astype(f32)
            final = rest - middle
            out_ref[i, rows_out:, lanes] = jnp.concatenate(
                [top, middle, final, jnp.zeros((13, LANES), f32)], axis=0
            ).astype(bf16)


def layer_norm(stream, gain_row, bias_row):
    center = jnp.mean(stream, axis=-1, keepdims=True)
    spread = jnp.mean(jnp.square(stream - center), axis=-1, keepdims=True)
    return (stream - center) * lax.rsqrt(spread + eps_norm) * gain_row + bias_row


def middle_kernel(
    part_ref, out_gain_ref, proj_ref, residual_ref, gain_ref, bias_ref, target_ref,
    middle_ref, outbound_ref, held_ref, sem_ref,
):
    sources, _, width = part_ref.shape
    copies = [
        pltpu.make_async_copy(
            proj_ref.at[pl.ds(t * width, width)], held_ref.at[pl.ds(t * width, width)], sem_ref.at[t]
        )
        for t in range(TP)
    ]
    for copy in copies:
        copy.start()
    rows = LANES
    heads = width // HEAD
    levels = jnp.sum(part_ref[:, rows:, :].astype(f32), axis=1)
    pieces = [levels[i * TP : (i + 1) * TP] for i in range(sources // TP)]
    highest = pieces[0]
    for piece in pieces[1:]:
        highest = jnp.maximum(highest, piece)
    shares = [jnp.exp2(piece - highest) for piece in pieces]
    whole = shares[0]
    for share in shares[1:]:
        whole = whole + share
    shares = jnp.concatenate([share / whole for share in shares], axis=0)
    columns = []
    for h in range(heads):
        square = jnp.concatenate(
            [
                shares[:, h * HEAD : (h + 1) * HEAD],
                jnp.zeros((LANES - sources, LANES), f32),
            ],
            axis=0,
        )
        columns.append(jnp.transpose(square))
    attended = []
    for t in range(TP):
        for h in range(heads):
            mixed = jnp.zeros((rows, HEAD), f32)
            for i in range(sources // TP):
                source = i * TP + t
                mixed = mixed + columns[h][:, source : source + 1] * part_ref[
                    source, :rows, h * HEAD : (h + 1) * HEAD
                ].astype(f32)
            attended.append(mixed.astype(bf16).astype(f32))
    attention = jnp.concatenate(attended, axis=1)
    mean_square = jnp.mean(attention * attention, axis=1, keepdims=True)
    scaled = (attention * out_gain_ref[...]).astype(bf16)
    projected = jnp.zeros((rows, held_ref.shape[1]), f32)
    for t in range(TP):
        copies[t].wait()
        lanes = slice(t * width, (t + 1) * width)
        projected = projected + jnp.dot(
            scaled[:, lanes], held_ref[lanes, :], preferred_element_type=f32
        )
    projected = projected * lax.rsqrt(mean_square + eps_norm)
    middle = layer_norm(
        alpha_mix * residual_ref[...].astype(f32) + projected, gain_ref[...], bias_ref[...]
    ).astype(bf16)
    middle_ref[...] = middle
    cut = middle.shape[1] // PARTS
    stacked = jnp.concatenate([middle[:, p * cut : (p + 1) * cut] for p in range(PARTS)], axis=0)
    out_rows = outbound_ref.shape[0]
    count = 4
    some = out_rows // count
    for c in range(count):
        row = c * some + lax.broadcasted_iota(jnp.int32, (some, PARTS * rows), 0)
        part = (row // CAPACITY) % PARTS
        slot = (row // (CAPACITY * PARTS)) * CAPACITY + row % CAPACITY
        lane = lax.broadcasted_iota(jnp.int32, (some, PARTS * rows), 1)
        code = jnp.where(part == lane // rows, slot, -1)
        chosen = (code == target_ref[0:1, :]) | (code == target_ref[1:2, :])
        outbound_ref[c * some : (c + 1) * some, :] = jnp.dot(
            jnp.where(chosen, 1.0, 0.0).astype(bf16), stacked, preferred_element_type=f32
        ).astype(bf16)


def swap_matrix(size):
    group = CAPACITY * PARTS
    tiles = size // group
    row = lax.broadcasted_iota(jnp.int32, (size, size), 0)
    col = lax.broadcasted_iota(jnp.int32, (size, size), 1)
    part = row // (tiles * CAPACITY)
    tile = (row // CAPACITY) % tiles
    inner = row % CAPACITY
    return jnp.where(col == tile * group + part * CAPACITY + inner, 1.0, 0.0).astype(bf16)


def expert_kernel(arrived_ref, gate_ref, up_ref, down_ref, served_ref, rows_ref, swap_ref):
    chunk = 256
    chunks = arrived_ref.shape[0] // chunk
    cut = arrived_ref.shape[1]
    some = chunk // PARTS
    swap_ref[...] = swap_matrix(chunk)
    for c in range(chunks):
        sorted_rows = jnp.dot(
            swap_ref[...], arrived_ref[c * chunk : (c + 1) * chunk, :], preferred_element_type=f32
        ).astype(bf16)
        for p in range(PARTS):
            rows_ref[c * some : (c + 1) * some, p * cut : (p + 1) * cut] = sorted_rows[
                p * some : (p + 1) * some
            ]
    rows = rows_ref[...]
    gate = jnp.dot(rows, gate_ref[...], preferred_element_type=f32)
    up = jnp.dot(rows, up_ref[...], preferred_element_type=f32)
    hidden = (gate / (1.0 + jnp.exp(-gate)) * up).astype(bf16)
    rows_ref[...] = jnp.dot(hidden, down_ref[...], preferred_element_type=f32).astype(bf16)
    for c in range(chunks):
        stacked = jnp.concatenate(
            [
                rows_ref[c * some : (c + 1) * some, p * cut : (p + 1) * cut]
                for p in range(PARTS)
            ],
            axis=0,
        )
        served_ref[c * chunk : (c + 1) * chunk, :] = lax.dot_general(
            swap_ref[...], stacked, (((0,), (0,)), ((), ())), preferred_element_type=f32
        ).astype(bf16)


def final_kernel(
    returned_ref, target_ref, weight_ref, middle_ref, gain_ref, bias_ref, out_ref, rows_ref
):
    chunk = 256
    chunks = returned_ref.shape[0] // chunk
    cut = returned_ref.shape[1]
    some = chunk // PARTS
    swap = swap_matrix(chunk)
    for c in range(chunks):
        sorted_rows = jnp.dot(
            swap, returned_ref[c * chunk : (c + 1) * chunk, :], preferred_element_type=f32
        ).astype(bf16)
        for p in range(PARTS):
            rows_ref[c * some : (c + 1) * some, p * cut : (p + 1) * cut] = sorted_rows[
                p * some : (p + 1) * some
            ]
    rows = middle_ref.shape[0]
    slot = lax.broadcasted_iota(jnp.int32, (rows, rows_ref.shape[0]), 1)
    chosen = jnp.concatenate(
        [jnp.where(slot == target_ref[:, k : k + 1], 1.0, 0.0) for k in range(2)], axis=0
    ).astype(bf16)
    picked = jnp.dot(chosen, rows_ref[...], preferred_element_type=f32)
    routed = picked[:rows] * weight_ref[:, 0:1] + picked[rows:] * weight_ref[:, 1:2]
    out_ref[...] = layer_norm(
        alpha_mix * middle_ref[...].astype(f32) + routed, gain_ref[...], bias_ref[...]
    ).astype(bf16)


def whole_vmem():
    return pl.BlockSpec(memory_space=pltpu.VMEM)


def in_hbm():
    return pl.BlockSpec(memory_space=pltpu.HBM)


def held(array):
    return pltpu.with_memory_space_constraint(array, pltpu.HBM)


def in_smem():
    return pl.BlockSpec(memory_space=pltpu.SMEM)


def params(mib, grid=0):
    more = {"dimension_semantics": ("arbitrary",)} if grid else {}
    return pltpu.CompilerParams(vmem_limit_bytes=mib << 20, **more)


def merge_kernel(own_any, other_any, out_hbm, own_ref, other_ref, out_ref, sems):
    blocks = out_ref.shape[0]
    rows = LANES
    heads = out_ref.shape[2] // HEAD
    arriving = [
        pltpu.make_async_copy(own_any.at[pl.ds(blocks, blocks)], own_ref, sems.at[0]),
        pltpu.make_async_copy(other_any.at[pl.ds(0, blocks)], other_ref, sems.at[1]),
    ]
    for copy in arriving:
        copy.start()
    for copy in arriving:
        copy.wait()
    flats = [
        jnp.sum(ref[:, rows:, :].astype(f32), axis=1) for ref in (own_ref, other_ref)
    ]
    upper = jnp.maximum(flats[0], flats[1])
    parts = [jnp.exp2(flat - upper) for flat in flats]
    both = parts[0] + parts[1]
    flat = upper + jnp.log2(both)
    top = flat.astype(bf16).astype(f32)
    rest = flat - top
    middle = rest.astype(bf16).astype(f32)
    final = rest - middle
    for h in range(heads):
        lanes = slice(h * HEAD, (h + 1) * HEAD)
        shares = jnp.concatenate(
            [(part / both)[:, lanes] for part in parts]
            + [jnp.zeros((LANES - 2 * blocks, LANES), f32)],
            axis=0,
        )
        columns = jnp.transpose(shares)
        for i in range(blocks):
            out_ref[i, :rows, lanes] = (
                own_ref[i, :rows, lanes].astype(f32) * columns[:, i : i + 1]
                + other_ref[i, :rows, lanes].astype(f32) * columns[:, blocks + i : blocks + i + 1]
            ).astype(bf16)
            out_ref[i, rows:, lanes] = jnp.concatenate(
                [
                    top[i : i + 1, lanes], middle[i : i + 1, lanes], final[i : i + 1, lanes],
                    jnp.zeros((13, LANES), f32),
                ],
                axis=0,
            ).astype(bf16)
    leaving = pltpu.make_async_copy(out_ref, out_hbm, sems.at[2])
    leaving.start()
    leaving.wait()


def attention_call(query_gain, key_gain, shared_rot, kv_parts):
    heads, all_rows, depth = shared_rot.shape
    tok_rows = kv_parts[0].shape[1]
    tile = TILE
    width = heads * HEAD
    steps = all_rows // tile
    out_block = pl.BlockSpec((tile // LANES, LANES + 16, width), lambda i: (i, 0, 0))
    return pl.pallas_call(
        attention_kernel,
        grid=(steps,),
        out_shape=pltpu.HBM((all_rows // LANES, LANES + 16, width), bf16),
        in_specs=[whole_vmem(), whole_vmem(), in_hbm()] + [pl.BlockSpec(memory_space=pl.ANY)] * SHARDS,
        out_specs=out_block,
        scratch_shapes=[
            pltpu.VMEM((SHARDS, depth, tok_rows), bf16),
            pltpu.VMEM((SHARDS, tok_rows, HEAD), bf16),
            pltpu.SMEM((SHARDS,), jnp.int32),
            pltpu.SMEM((SHARDS,), jnp.int32),
            pltpu.SMEM((SHARDS,), jnp.int32),
            pltpu.SMEM((1,), jnp.int32),
            pltpu.VMEM((heads * tile, HEAD), f32),
            pltpu.VMEM((heads * tile, HEAD), f32),
            pltpu.VMEM((heads * tile, HEAD), f32),
            pltpu.VMEM((steps, heads, tile, depth), bf16),
            pltpu.SemaphoreType.DMA((steps,)),
            pltpu.SemaphoreType.DMA((SHARDS,)),
            pltpu.SemaphoreType.DMA((SHARDS * tok_rows // HEAD,)),
        ],
        compiler_params=params(40, 1),
        name="document_attention",
    )(
        query_gain.reshape(1, HEAD), key_gain.reshape(1, HEAD), held(shared_rot), *kv_parts,
    )


def per_device(
    queries, key_heads, value_heads, documents, query_gain, key_gain, out_gain, out_proj,
    residual, mid_gain, mid_bias, routes, route_weights, expert_gate, expert_up, expert_down,
    final_gain, final_bias,
):
    tok_rows, width = queries.shape
    heads = width // HEAD
    sp_size = lax.axis_size("sp")
    tp_size = lax.axis_size("tp")
    shards = sp_size // SHARE
    table = jnp.asarray(angle_tables(sp_size * tok_rows // GRID))
    index = lax.axis_index("sp").astype(jnp.int32).reshape(1)
    owner_groups = [
        [(g * SHARE + c + 2 * i) * tp_size + t for i in range(SHARE // 2) for t in range(tp_size)]
        for g in range(shards)
        for c in range(2)
    ]

    kv_rows = 2 * HEAD + MARKS
    kv, marked = pl.pallas_call(
        key_kernel,
        out_shape=(
            pltpu.HBM((kv_rows, tok_rows), bf16),
            pltpu.HBM((tok_rows + MARKS, width), bf16),
        ),
        in_specs=[in_smem()] + [in_hbm()] * 6,
        out_specs=(in_hbm(), in_hbm()),
        scratch_shapes=[
            pltpu.VMEM(key_heads.shape, bf16),
            pltpu.VMEM(value_heads.shape, bf16),
            pltpu.VMEM((1, tok_rows), jnp.int32),
            pltpu.VMEM((1, HEAD), f32),
            pltpu.VMEM(table.shape, f32),
            pltpu.VMEM((kv_rows, tok_rows), bf16),
            pltpu.VMEM((tok_rows + MARKS, width), bf16),
            pltpu.SemaphoreType.DMA((6,)),
            pltpu.SemaphoreType.DMA((2,)),
        ],
        compiler_params=params(16),
        name="key_rotation",
    )(
        index, held(key_heads), held(value_heads), held(documents.reshape(1, tok_rows)),
        held(key_gain.reshape(1, HEAD)), held(table), held(queries),
    )

    def moved(array, dz, dy):
        pairs = []
        for z in range(4):
            for y in range(4):
                for c in range(2):
                    way = 1 - 2 * c
                    goal = ((z + way * dz) % 4) * 8 + ((y + way * dy) % 4) * 2 + c
                    pairs.append((z * 8 + y * 2 + c, goal))
        return lax.ppermute(array, "sp", pairs)

    across = moved(kv, 0, 2)
    after = moved(kv, 1, 0)
    ahead = moved(kv, -1, 0)
    beyond = moved(after, 1, 0)
    after_across = moved(across, 1, 0)
    ahead_across = moved(across, -1, 0)
    beyond_across = moved(after_across, 1, 0)
    kv_parts = [kv, after, ahead, across, beyond, after_across, ahead_across, beyond_across]

    beside = lax.ppermute(marked, "sp", [(i, i ^ 2) for i in range(sp_size)])
    shared = [marked]
    for array in (marked, beside):
        shared.append(lax.ppermute(array, "sp", [(i, i ^ 1) for i in range(sp_size)]))
    shared.insert(2, beside)

    shared_rot = pl.pallas_call(
        query_kernel,
        out_shape=pltpu.HBM((heads, SHARE * tok_rows, 2 * HEAD), bf16),
        in_specs=[in_smem()] + [pl.BlockSpec(memory_space=pl.ANY)] * SHARE + [in_hbm()] * 2,
        out_specs=in_hbm(),
        scratch_shapes=[
            pltpu.VMEM((heads, SHARE * tok_rows, 2 * HEAD), bf16),
            pltpu.VMEM((1, HEAD), f32),
            pltpu.VMEM(table.shape, f32),
            pltpu.VMEM((SHARE,) + marked.shape, bf16),
            pltpu.SemaphoreType.DMA((heads,)),
            pltpu.SemaphoreType.DMA((2 + SHARE,)),
        ],
        compiler_params=params(24),
        name="query_rotation",
    )(index, held(marked), *shared[1:], held(query_gain.reshape(1, HEAD)), held(table))

    partial = attention_call(query_gain, key_gain, shared_rot, kv_parts)
    other = lax.ppermute(partial, "sp", [(i, i ^ 1) for i in range(sp_size)])
    blocks = partial.shape[0] // 2
    block = (blocks,) + partial.shape[1:]
    partial = pl.pallas_call(
        merge_kernel,
        out_shape=pltpu.HBM(block, bf16),
        in_specs=[pl.BlockSpec(memory_space=pl.ANY)] * 2,
        out_specs=in_hbm(),
        scratch_shapes=[
            pltpu.VMEM(block, bf16), pltpu.VMEM(block, bf16), pltpu.VMEM(block, bf16),
            pltpu.SemaphoreType.DMA((3,)),
        ],
        compiler_params=params(16),
        name="merge_parts",
    )(held(partial), other)
    partial = lax.all_to_all(
        partial, ("sp", "tp"), 0, 0, tiled=True, axis_index_groups=owner_groups
    )

    out_rows, model_width = residual.shape
    expert_total = sp_size * tp_size
    flat = routes.T.reshape(-1)
    order = jnp.arange(flat.shape[0], dtype=jnp.int32)
    earlier = (flat[:, None] == flat[None, :]) & (order[None, :] < order[:, None])
    rank = jnp.sum(earlier.astype(jnp.int32), axis=1)
    target = (flat * CAPACITY + rank).reshape(2, out_rows)

    cut = model_width // PARTS
    exchange_rows = expert_total * CAPACITY * PARTS
    middle, outbound = pl.pallas_call(
        middle_kernel,
        out_shape=(
            jax.ShapeDtypeStruct((out_rows, model_width), bf16),
            jax.ShapeDtypeStruct((exchange_rows, cut), bf16),
        ),
        in_specs=[
            whole_vmem(), whole_vmem(), in_hbm(), whole_vmem(),
            whole_vmem(), whole_vmem(), whole_vmem(),
        ],
        out_specs=(whole_vmem(), whole_vmem()),
        scratch_shapes=[
            pltpu.VMEM(out_proj.shape, bf16),
            pltpu.SemaphoreType.DMA((TP,)),
        ],
        compiler_params=params(40),
        name="middle_stream",
    )(
        partial, out_gain.reshape(1, -1), held(out_proj), residual, mid_gain.reshape(1, -1),
        mid_bias.reshape(1, -1), jnp.tile(target, (1, PARTS)),
    )
    arrived = lax.all_to_all(
        outbound.reshape(expert_total, CAPACITY * PARTS, cut), ("sp", "tp"), 0, 0, tiled=True
    )
    hidden_width = expert_gate.shape[2]
    served = pl.pallas_call(
        expert_kernel,
        out_shape=jax.ShapeDtypeStruct((exchange_rows, cut), bf16),
        in_specs=[whole_vmem() for _ in range(4)],
        out_specs=whole_vmem(),
        scratch_shapes=[
            pltpu.VMEM((expert_total * CAPACITY, model_width), bf16),
            pltpu.VMEM((256, 256), bf16),
        ],
        compiler_params=params(40),
        name="expert",
    )(
        arrived.reshape(exchange_rows, cut),
        expert_gate.reshape(model_width, hidden_width),
        expert_up.reshape(model_width, hidden_width),
        expert_down.reshape(hidden_width, model_width),
    )
    returned = lax.all_to_all(
        served.reshape(expert_total, CAPACITY * PARTS, cut), ("sp", "tp"), 0, 0, tiled=True
    )
    return pl.pallas_call(
        final_kernel,
        out_shape=jax.ShapeDtypeStruct((out_rows, model_width), bf16),
        in_specs=[whole_vmem() for _ in range(6)],
        out_specs=whole_vmem(),
        scratch_shapes=[pltpu.VMEM((expert_total * CAPACITY, model_width), bf16)],
        compiler_params=params(40),
        name="final_stream",
    )(
        returned.reshape(exchange_rows, cut), target.T, route_weights, middle,
        final_gain.reshape(1, -1), final_bias.reshape(1, -1),
    )


def solution(mesh):
    rows = P(("sp", "tp"), None)
    experts = P(("sp", "tp"), None, None)
    return jax.shard_map(
        per_device,
        mesh=mesh,
        in_specs=(
            P("sp", "tp"), P("sp", "tp"), P("sp", "tp"), P("sp"), P(), P(), P(), P(), rows, P(),
            P(), rows, rows, experts, experts, experts, P(), P(),
        ),
        out_specs=rows,
        check_vma=False,
    )
```

```python
import numpy as np

import jax
import jax.numpy as jnp
from jax import lax
from jax.experimental import pallas as pl
from jax.experimental.pallas import tpu as pltpu
from jax.sharding import PartitionSpec as P

HEAD = 128
GRID = 64
TP = 4
SHARE = 4
LANES = 128
TILE = 2048
APART = 32768.0
CAPACITY = 4
PARTS = 4
SHARDS = 8
MARKS = 16

eps_norm = 1e-06
alpha_mix = 8.0**0.25
theta_base = 10000.0
score_scale = HEAD**-0.5 * 1.4426950408889634
f32 = jnp.float32
bf16 = jnp.bfloat16


def angle_tables(row_count):
    pair_count = HEAD // 4
    inv_freq = np.power(
        np.float32(theta_base), -np.arange(pair_count, dtype=np.float32) / np.float32(pair_count)
    ).astype(np.float32)

    def both(count):
        angles = (np.arange(count, dtype=np.float32)[:, None] * inv_freq[None, :]).astype(np.float32)
        return np.cos(angles.astype(np.float64)), np.sin(angles.astype(np.float64))

    row_cos, row_sin = both(row_count)
    col_cos, col_sin = both(GRID)
    none_row, none_col = np.zeros_like(row_cos), np.zeros_like(col_cos)
    row_c = np.concatenate([row_cos, none_row, row_cos, none_row], axis=1)
    row_s = np.concatenate([-row_sin, none_row, row_sin, none_row], axis=1)
    col_c = np.concatenate([none_col, col_cos, none_col, col_cos], axis=1)
    col_s = np.concatenate([none_col, -col_sin, none_col, col_sin], axis=1)
    return np.concatenate([row_c, row_s, col_c, col_s], axis=0).astype(np.float32)


def tables_at(table_ref, first, grid_rows):
    row_count = (table_ref.shape[0] - 2 * GRID) // 2

    def table_of(row_first, col_first):
        row_part = table_ref[pl.ds(pl.multiple_of(row_first, 8), grid_rows)]
        col_part = table_ref[col_first : col_first + GRID]
        return (row_part[:, None, :] + col_part[None, :, :]).reshape(grid_rows * GRID, HEAD)

    return (
        table_of(first, 2 * row_count),
        table_of(row_count + first, 2 * row_count + GRID),
    )


def normed_rotated(values, gain_row, cosine, sine):
    inv_rms = lax.rsqrt(jnp.mean(values * values, axis=-1, keepdims=True) + eps_norm)
    values = values * inv_rms * gain_row
    return (values * cosine + pltpu.roll(values, HEAD // 2, 1) * sine).astype(bf16)


def key_kernel(
    index_ref, key_hbm, value_hbm, doc_hbm, gain_hbm, table_hbm, query_hbm, out_hbm, marked_hbm,
    key_ref, value_ref, doc_ref, gain_ref, table_ref, built_ref, lines_ref, in_sems, out_sems,
):
    tok_rows, width = query_hbm.shape
    passing = pltpu.make_async_copy(query_hbm, lines_ref.at[pl.ds(0, tok_rows)], in_sems.at[5])
    pairs = (
        (key_hbm, key_ref), (value_hbm, value_ref), (doc_hbm, doc_ref), (gain_hbm, gain_ref),
        (table_hbm, table_ref),
    )
    arriving = [pltpu.make_async_copy(a, b, in_sems.at[i]) for i, (a, b) in enumerate(pairs)]
    for copy in arriving:
        copy.start()
    passing.start()
    for copy in arriving:
        copy.wait()
    grid_rows = tok_rows // GRID
    cosine, sine = tables_at(table_ref, index_ref[0] * grid_rows, grid_rows)
    rotated = normed_rotated(key_ref[...].astype(f32), gain_ref[...], cosine, sine)
    numbers = lax.broadcasted_iota(jnp.int32, (MARKS, tok_rows), 0)
    documents = doc_ref[...]
    marks = jnp.where(numbers == documents, 1.0, 0.0)
    marks = jnp.where(numbers == MARKS - 1, documents.astype(f32), marks).astype(bf16)
    built_ref[:HEAD, :] = jnp.transpose(rotated.astype(f32)).astype(bf16)
    built_ref[HEAD : HEAD + MARKS, :] = marks
    for g in range(tok_rows // HEAD):
        built_ref[HEAD + MARKS :, g * HEAD : (g + 1) * HEAD] = value_ref[
            g * HEAD : (g + 1) * HEAD, :
        ]
    leaving = pltpu.make_async_copy(built_ref, out_hbm, out_sems.at[0])
    leaving.start()
    lines = [
        documents[:, i * width : (i + 1) * width].astype(f32) for i in range(tok_rows // width)
    ]
    lines.append(jnp.zeros((MARKS - len(lines), width), f32))
    lines_ref[tok_rows:, :] = jnp.concatenate(lines, axis=0).astype(bf16)
    passing.wait()
    marking = pltpu.make_async_copy(lines_ref, marked_hbm, out_sems.at[1])
    marking.start()
    leaving.wait()
    marking.wait()


def query_kernel(index_ref, *refs):
    query_hbms = refs[:SHARE]
    (
        gain_hbm, table_hbm, out_ref, gain_ref, table_ref, query_refs, in_sems,
    ) = refs[SHARE:]
    arriving = [
        pltpu.make_async_copy(query_hbm, query_refs.at[i], in_sems.at[2 + i])
        for i, query_hbm in enumerate(query_hbms)
    ] + [
        pltpu.make_async_copy(gain_hbm, gain_ref, in_sems.at[0]),
        pltpu.make_async_copy(table_hbm, table_ref, in_sems.at[1]),
    ]
    for copy in arriving:
        copy.start()
    for copy in arriving:
        copy.wait()
    tok_rows = query_refs.shape[1] - MARKS
    width = query_refs.shape[2]
    grid_rows = tok_rows // GRID
    own = index_ref[0] % SHARE
    numbers = lax.broadcasted_iota(jnp.int32, (LANES, tok_rows), 0).astype(f32)
    for i in range(SHARE):
        query_ref = query_refs.at[i]
        place = own ^ i
        cosine, sine = tables_at(
            table_ref, (index_ref[0] - own + place) * grid_rows, grid_rows
        )
        lines = query_ref[tok_rows:, :].astype(f32)
        documents = jnp.concatenate([lines[k : k + 1] for k in range(tok_rows // width)], axis=1)
        apart = jnp.where(numbers == documents, 0.0, -APART)
        apart = jnp.where(numbers >= MARKS - 2, 0.0, apart)
        apart = jnp.where(numbers == MARKS - 2, documents, apart)
        apart = jnp.transpose(apart).astype(bf16)
        half = 0 if i % 2 else SHARE // 2
        rows = pl.ds(pl.multiple_of((half + place // 2) * tok_rows, tok_rows), tok_rows)
        for h in range(out_ref.shape[0]):
            values = query_ref[:tok_rows, h * HEAD : (h + 1) * HEAD].astype(f32)
            out_ref[h, rows, :HEAD] = normed_rotated(values, gain_ref[...], cosine, sine)
            out_ref[h, rows, HEAD:] = apart


def attention_kernel(query_gain_ref, key_gain_ref, query_ref, *refs):
    kv_refs = refs[:SHARDS]
    refs = refs[SHARDS:]
    (
        partner_ref, own_ref, keys_ref, values_ref, first_ref, last_ref, order_ref, small_ref, acc_ref, total_ref, max_ref,
        key_sems, value_sems,
    ) = refs
    heads, all_rows, depth = query_ref.shape
    tok_rows = keys_ref.shape[2]
    rows = acc_ref.shape[0]
    tile = rows // heads
    marked = HEAD + MARKS
    groups = tok_rows // HEAD
    step = pl.program_id(0)

    @pl.when(step == 0)
    def fetch():
        arriving = []
        for j, kv_ref in enumerate(kv_refs):
            arriving.append(
                pltpu.make_async_copy(
                    kv_ref.at[pl.ds(0, marked)], keys_ref.at[j, pl.ds(0, marked)], key_sems.at[j]
                )
            )
        for j, kv_ref in enumerate(kv_refs):
            for g in range(groups):
                arriving.append(
                    pltpu.make_async_copy(
                        kv_ref.at[pl.ds(marked, HEAD), pl.ds(g * HEAD, HEAD)],
                        values_ref.at[j, pl.ds(g * HEAD, HEAD)],
                        value_sems.at[j * groups + g],
                    )
                )
        for copy in arriving:
            copy.start()
        largest = jnp.max(jnp.abs(query_gain_ref[...])) * jnp.max(jnp.abs(key_gain_ref[...]))
        small_ref[0] = (largest * (HEAD * score_scale * 1.02) < 50.0).astype(jnp.int32)
        for j in range(SHARDS):
            keys_ref[j, marked:, :] = jnp.zeros((depth - marked, tok_rows), bf16)
        for copy in arriving:
            copy.wait()
        for j in range(SHARDS):
            line = keys_ref[j, HEAD:marked, :].astype(f32)
            first_ref[j] = line[MARKS - 1, 0].astype(jnp.int32)
            last_ref[j] = line[MARKS - 1, tok_rows - 1].astype(jnp.int32)

    queries = query_ref[...].reshape(rows, depth)
    low = jnp.int32(1 << 20)
    high = jnp.int32(-1)
    half = all_rows // 2
    for begin in range(0, tile, half):
        top = query_ref[0, begin : begin + 16, HEAD:].astype(f32)
        bottom = query_ref[0, begin + half - 16 : begin + half, HEAD:].astype(f32)
        low = jnp.minimum(low, top[0, MARKS - 2].astype(jnp.int32))
        high = jnp.maximum(high, bottom[15, MARKS - 2].astype(jnp.int32))
    count = jnp.int32(0)
    for j in range(SHARDS):
        order_ref[count] = jnp.int32(j)
        count += ((first_ref[j] <= high) & (last_ref[j] >= low)).astype(jnp.int32)

    acc_ref[...] = jnp.zeros_like(acc_ref)
    total_ref[...] = jnp.zeros_like(total_ref)

    def scores_of(j):
        return jnp.dot(queries, keys_ref[j], preferred_element_type=f32)

    def folded(weights):
        part = weights[:, :LANES]
        for i in range(1, weights.shape[1] // LANES):
            part = part + weights[:, i * LANES : (i + 1) * LANES]
        return part

    @pl.when(small_ref[0] == 1)
    def without_max():
        max_ref[...] = jnp.zeros_like(max_ref)

        def advance(i, unused):
            j = order_ref[i]
            weights = jnp.exp2(scores_of(j) * score_scale)
            total_ref[...] += folded(weights)
            acc_ref[...] += jnp.dot(
                weights.astype(bf16), values_ref[j], preferred_element_type=f32
            )
            return unused

        lax.fori_loop(0, count, advance, 0)

    @pl.when(small_ref[0] == 0)
    def with_max():
        max_ref[...] = jnp.full_like(max_ref, -1e30)

        some_rows = 512

        def advance(i, unused):
            j = order_ref[i]

            def some_of(r, unused):
                mine = pl.ds(pl.multiple_of((r % (tile // some_rows)) * some_rows, some_rows), some_rows)
                held = pl.ds(pl.multiple_of(r * some_rows, some_rows), some_rows)
                part = query_ref[r // (tile // some_rows), mine, :]
                scores = jnp.dot(part, keys_ref[j], preferred_element_type=f32) * score_scale
                old_max = max_ref[held]
                new_max = jnp.maximum(old_max, jnp.max(scores, axis=1, keepdims=True))
                weights = jnp.exp2(scores - new_max[:, :1])
                rescale = jnp.exp2(old_max - new_max)
                max_ref[held] = new_max
                total_ref[held] = total_ref[held] * rescale + folded(weights)
                acc_ref[held] = acc_ref[held] * rescale + jnp.dot(
                    weights.astype(bf16), values_ref[j], preferred_element_type=f32
                )
                return unused

            return lax.fori_loop(0, rows // some_rows, some_of, unused)

        lax.fori_loop(0, count, advance, 0)

    rows_out = LANES
    eye = lax.broadcasted_iota(jnp.int32, (rows_out, LANES), 0) == lax.broadcasted_iota(
        jnp.int32, (rows_out, LANES), 1
    )
    blocks = tile // rows_out
    for h in range(heads):
        for i in range(blocks):
            out_ref = partner_ref.at[i] if i < blocks // 2 else own_ref.at[i - blocks // 2]
            mine = slice(h * tile + i * rows_out, h * tile + (i + 1) * rows_out)
            lanes = slice(h * HEAD, (h + 1) * HEAD)
            total = jnp.sum(total_ref[mine], axis=1, keepdims=True)
            some = total > 0.0
            kept = jnp.where(some, total, 1.0)
            level = jnp.where(some, max_ref[mine] + jnp.log2(kept), -1e30)
            share = 1.0 / kept
            mixed = acc_ref[mine] * share
            out_ref[:rows_out, lanes] = mixed.astype(bf16)
            flat = jnp.sum(jnp.where(eye, level, 0.0), axis=0, keepdims=True)
            top = flat.astype(bf16).astype(f32)
            rest = flat - top
            middle = rest.astype(bf16).astype(f32)
            final = rest - middle
            out_ref[rows_out:, lanes] = jnp.concatenate(
                [top, middle, final, jnp.zeros((13, LANES), f32)], axis=0
            ).astype(bf16)


def layer_norm(stream, gain_row, bias_row):
    center = jnp.mean(stream, axis=-1, keepdims=True)
    spread = jnp.mean(jnp.square(stream - center), axis=-1, keepdims=True)
    return (stream - center) * lax.rsqrt(spread + eps_norm) * gain_row + bias_row


def middle_kernel(
    part_ref, out_gain_ref, proj_ref, residual_ref, gain_ref, bias_ref, target_ref,
    middle_ref, outbound_ref, held_ref, sem_ref,
):
    sources, _, width = part_ref.shape
    copies = [
        pltpu.make_async_copy(
            proj_ref.at[pl.ds(t * width, width)], held_ref.at[pl.ds(t * width, width)], sem_ref.at[t]
        )
        for t in range(TP)
    ]
    for copy in copies:
        copy.start()
    rows = LANES
    heads = width // HEAD
    levels = jnp.sum(part_ref[:, rows:, :].astype(f32), axis=1)
    pieces = [levels[i * TP : (i + 1) * TP] for i in range(sources // TP)]
    highest = pieces[0]
    for piece in pieces[1:]:
        highest = jnp.maximum(highest, piece)
    shares = [jnp.exp2(piece - highest) for piece in pieces]
    whole = shares[0]
    for share in shares[1:]:
        whole = whole + share
    shares = jnp.concatenate([share / whole for share in shares], axis=0)
    columns = []
    for h in range(heads):
        square = jnp.concatenate(
            [
                shares[:, h * HEAD : (h + 1) * HEAD],
                jnp.zeros((LANES - sources, LANES), f32),
            ],
            axis=0,
        )
        columns.append(jnp.transpose(square))
    attended = []
    for t in range(TP):
        for h in range(heads):
            mixed = jnp.zeros((rows, HEAD), f32)
            for i in range(sources // TP):
                source = i * TP + t
                mixed = mixed + columns[h][:, source : source + 1] * part_ref[
                    source, :rows, h * HEAD : (h + 1) * HEAD
                ].astype(f32)
            attended.append(mixed.astype(bf16).astype(f32))
    attention = jnp.concatenate(attended, axis=1)
    mean_square = jnp.mean(attention * attention, axis=1, keepdims=True)
    scaled = (attention * out_gain_ref[...]).astype(bf16)
    projected = jnp.zeros((rows, held_ref.shape[1]), f32)
    for t in range(TP):
        copies[t].wait()
        lanes = slice(t * width, (t + 1) * width)
        projected = projected + jnp.dot(
            scaled[:, lanes], held_ref[lanes, :], preferred_element_type=f32
        )
    projected = projected * lax.rsqrt(mean_square + eps_norm)
    middle = layer_norm(
        alpha_mix * residual_ref[...].astype(f32) + projected, gain_ref[...], bias_ref[...]
    ).astype(bf16)
    middle_ref[...] = middle
    cut = middle.shape[1] // PARTS
    stacked = jnp.concatenate([middle[:, p * cut : (p + 1) * cut] for p in range(PARTS)], axis=0)
    out_rows = outbound_ref.shape[0]
    count = 4
    some = out_rows // count
    for c in range(count):
        row = c * some + lax.broadcasted_iota(jnp.int32, (some, PARTS * rows), 0)
        part = (row // CAPACITY) % PARTS
        slot = (row // (CAPACITY * PARTS)) * CAPACITY + row % CAPACITY
        lane = lax.broadcasted_iota(jnp.int32, (some, PARTS * rows), 1)
        code = jnp.where(part == lane // rows, slot, -1)
        chosen = (code == target_ref[0:1, :]) | (code == target_ref[1:2, :])
        outbound_ref[c * some : (c + 1) * some, :] = jnp.dot(
            jnp.where(chosen, 1.0, 0.0).astype(bf16), stacked, preferred_element_type=f32
        ).astype(bf16)


def swap_matrix(size):
    group = CAPACITY * PARTS
    tiles = size // group
    row = lax.broadcasted_iota(jnp.int32, (size, size), 0)
    col = lax.broadcasted_iota(jnp.int32, (size, size), 1)
    part = row // (tiles * CAPACITY)
    tile = (row // CAPACITY) % tiles
    inner = row % CAPACITY
    return jnp.where(col == tile * group + part * CAPACITY + inner, 1.0, 0.0).astype(bf16)


def expert_kernel(arrived_ref, gate_ref, up_ref, down_ref, served_ref, rows_ref, swap_ref):
    chunk = 256
    chunks = arrived_ref.shape[0] // chunk
    cut = arrived_ref.shape[1]
    some = chunk // PARTS
    swap_ref[...] = swap_matrix(chunk)
    for c in range(chunks):
        sorted_rows = jnp.dot(
            swap_ref[...], arrived_ref[c * chunk : (c + 1) * chunk, :], preferred_element_type=f32
        ).astype(bf16)
        for p in range(PARTS):
            rows_ref[c * some : (c + 1) * some, p * cut : (p + 1) * cut] = sorted_rows[
                p * some : (p + 1) * some
            ]
    rows = rows_ref[...]
    gate = jnp.dot(rows, gate_ref[...], preferred_element_type=f32)
    up = jnp.dot(rows, up_ref[...], preferred_element_type=f32)
    hidden = (gate / (1.0 + jnp.exp(-gate)) * up).astype(bf16)
    rows_ref[...] = jnp.dot(hidden, down_ref[...], preferred_element_type=f32).astype(bf16)
    for c in range(chunks):
        stacked = jnp.concatenate(
            [
                rows_ref[c * some : (c + 1) * some, p * cut : (p + 1) * cut]
                for p in range(PARTS)
            ],
            axis=0,
        )
        served_ref[c * chunk : (c + 1) * chunk, :] = lax.dot_general(
            swap_ref[...], stacked, (((0,), (0,)), ((), ())), preferred_element_type=f32
        ).astype(bf16)


def final_kernel(
    returned_ref, target_ref, weight_ref, middle_ref, gain_ref, bias_ref, out_ref, rows_ref
):
    chunk = 256
    chunks = returned_ref.shape[0] // chunk
    cut = returned_ref.shape[1]
    some = chunk // PARTS
    swap = swap_matrix(chunk)
    for c in range(chunks):
        sorted_rows = jnp.dot(
            swap, returned_ref[c * chunk : (c + 1) * chunk, :], preferred_element_type=f32
        ).astype(bf16)
        for p in range(PARTS):
            rows_ref[c * some : (c + 1) * some, p * cut : (p + 1) * cut] = sorted_rows[
                p * some : (p + 1) * some
            ]
    rows = middle_ref.shape[0]
    slot = lax.broadcasted_iota(jnp.int32, (rows, rows_ref.shape[0]), 1)
    chosen = jnp.concatenate(
        [jnp.where(slot == target_ref[:, k : k + 1], 1.0, 0.0) for k in range(2)], axis=0
    ).astype(bf16)
    picked = jnp.dot(chosen, rows_ref[...], preferred_element_type=f32)
    routed = picked[:rows] * weight_ref[:, 0:1] + picked[rows:] * weight_ref[:, 1:2]
    out_ref[...] = layer_norm(
        alpha_mix * middle_ref[...].astype(f32) + routed, gain_ref[...], bias_ref[...]
    ).astype(bf16)


def whole_vmem():
    return pl.BlockSpec(memory_space=pltpu.VMEM)


def in_hbm():
    return pl.BlockSpec(memory_space=pltpu.HBM)


def held(array):
    return pltpu.with_memory_space_constraint(array, pltpu.HBM)


def in_smem():
    return pl.BlockSpec(memory_space=pltpu.SMEM)


def params(mib, grid=0):
    more = {"dimension_semantics": ("arbitrary",)} if grid else {}
    return pltpu.CompilerParams(vmem_limit_bytes=mib << 20, **more)


def merge_kernel(own_any, other_any, out_hbm, own_ref, other_ref, out_ref, sems):
    blocks = out_ref.shape[0]
    rows = LANES
    heads = out_ref.shape[2] // HEAD
    arriving = [
        pltpu.make_async_copy(own_any, own_ref, sems.at[0]),
        pltpu.make_async_copy(other_any, other_ref, sems.at[1]),
    ]
    for copy in arriving:
        copy.start()
    for copy in arriving:
        copy.wait()
    flats = [
        jnp.sum(ref[:, rows:, :].astype(f32), axis=1) for ref in (own_ref, other_ref)
    ]
    upper = jnp.maximum(flats[0], flats[1])
    parts = [jnp.exp2(flat - upper) for flat in flats]
    both = parts[0] + parts[1]
    flat = upper + jnp.log2(both)
    top = flat.astype(bf16).astype(f32)
    rest = flat - top
    middle = rest.astype(bf16).astype(f32)
    final = rest - middle
    for h in range(heads):
        lanes = slice(h * HEAD, (h + 1) * HEAD)
        shares = jnp.concatenate(
            [(part / both)[:, lanes] for part in parts]
            + [jnp.zeros((LANES - 2 * blocks, LANES), f32)],
            axis=0,
        )
        columns = jnp.transpose(shares)
        for i in range(blocks):
            out_ref[i, :rows, lanes] = (
                own_ref[i, :rows, lanes].astype(f32) * columns[:, i : i + 1]
                + other_ref[i, :rows, lanes].astype(f32) * columns[:, blocks + i : blocks + i + 1]
            ).astype(bf16)
            out_ref[i, rows:, lanes] = jnp.concatenate(
                [
                    top[i : i + 1, lanes], middle[i : i + 1, lanes], final[i : i + 1, lanes],
                    jnp.zeros((13, LANES), f32),
                ],
                axis=0,
            ).astype(bf16)
    leaving = pltpu.make_async_copy(out_ref, out_hbm, sems.at[2])
    leaving.start()
    leaving.wait()


def attention_call(query_gain, key_gain, shared_rot, kv_parts):
    heads, all_rows, depth = shared_rot.shape
    tok_rows = kv_parts[0].shape[1]
    tile = TILE
    width = heads * HEAD
    steps = all_rows // tile
    half_shape = (tile // LANES // 2, LANES + 16, width)
    half_block = pl.BlockSpec(half_shape, lambda i: (0, 0, 0))
    return pl.pallas_call(
        attention_kernel,
        grid=(steps,),
        out_shape=(pltpu.HBM(half_shape, bf16), pltpu.HBM(half_shape, bf16)),
        in_specs=[whole_vmem(), whole_vmem(), whole_vmem()] + [pl.BlockSpec(memory_space=pl.ANY)] * SHARDS,
        out_specs=(half_block, half_block),
        scratch_shapes=[
            pltpu.VMEM((SHARDS, depth, tok_rows), bf16),
            pltpu.VMEM((SHARDS, tok_rows, HEAD), bf16),
            pltpu.SMEM((SHARDS,), jnp.int32),
            pltpu.SMEM((SHARDS,), jnp.int32),
            pltpu.SMEM((SHARDS,), jnp.int32),
            pltpu.SMEM((1,), jnp.int32),
            pltpu.VMEM((heads * tile, HEAD), f32),
            pltpu.VMEM((heads * tile, HEAD), f32),
            pltpu.VMEM((heads * tile, HEAD), f32),
            pltpu.SemaphoreType.DMA((SHARDS,)),
            pltpu.SemaphoreType.DMA((SHARDS * tok_rows // HEAD,)),
        ],
        compiler_params=params(40, 1),
        name="document_attention",
    )(
        query_gain.reshape(1, HEAD), key_gain.reshape(1, HEAD), shared_rot, *kv_parts,
    )


def per_device(
    queries, key_heads, value_heads, documents, query_gain, key_gain, out_gain, out_proj,
    residual, mid_gain, mid_bias, routes, route_weights, expert_gate, expert_up, expert_down,
    final_gain, final_bias,
):
    tok_rows, width = queries.shape
    heads = width // HEAD
    sp_size = lax.axis_size("sp")
    tp_size = lax.axis_size("tp")
    shards = sp_size // SHARE
    table = jnp.asarray(angle_tables(sp_size * tok_rows // GRID))
    index = lax.axis_index("sp").astype(jnp.int32).reshape(1)
    owner_groups = [
        [(g * SHARE + c + 2 * i) * tp_size + t for i in range(SHARE // 2) for t in range(tp_size)]
        for g in range(shards)
        for c in range(2)
    ]

    kv_rows = 2 * HEAD + MARKS
    kv, marked = pl.pallas_call(
        key_kernel,
        out_shape=(
            pltpu.HBM((kv_rows, tok_rows), bf16),
            pltpu.HBM((tok_rows + MARKS, width), bf16),
        ),
        in_specs=[in_smem()] + [in_hbm()] * 6,
        out_specs=(in_hbm(), in_hbm()),
        scratch_shapes=[
            pltpu.VMEM(key_heads.shape, bf16),
            pltpu.VMEM(value_heads.shape, bf16),
            pltpu.VMEM((1, tok_rows), jnp.int32),
            pltpu.VMEM((1, HEAD), f32),
            pltpu.VMEM(table.shape, f32),
            pltpu.VMEM((kv_rows, tok_rows), bf16),
            pltpu.VMEM((tok_rows + MARKS, width), bf16),
            pltpu.SemaphoreType.DMA((6,)),
            pltpu.SemaphoreType.DMA((2,)),
        ],
        compiler_params=params(16),
        name="key_rotation",
    )(
        index, held(key_heads), held(value_heads), held(documents.reshape(1, tok_rows)),
        held(key_gain.reshape(1, HEAD)), held(table), held(queries),
    )

    def moved(array, dz, dy):
        pairs = []
        for z in range(4):
            for y in range(4):
                for c in range(2):
                    way = 1 - 2 * c
                    goal = ((z + way * dz) % 4) * 8 + ((y + way * dy) % 4) * 2 + c
                    pairs.append((z * 8 + y * 2 + c, goal))
        return lax.ppermute(array, "sp", pairs)

    across = moved(kv, 0, 2)
    after = moved(kv, 1, 0)
    ahead = moved(kv, -1, 0)
    beyond = moved(after, 1, 0)
    after_across = moved(across, 1, 0)
    ahead_across = moved(across, -1, 0)
    beyond_across = moved(after_across, 1, 0)
    kv_parts = [kv, after, ahead, across, beyond, after_across, ahead_across, beyond_across]

    beside = lax.ppermute(marked, "sp", [(i, i ^ 2) for i in range(sp_size)])
    shared = [marked]
    for array in (marked, beside):
        shared.append(lax.ppermute(array, "sp", [(i, i ^ 1) for i in range(sp_size)]))
    shared.insert(2, beside)

    shared_rot = pl.pallas_call(
        query_kernel,
        out_shape=jax.ShapeDtypeStruct((heads, SHARE * tok_rows, 2 * HEAD), bf16),
        in_specs=[in_smem()] + [pl.BlockSpec(memory_space=pl.ANY)] * SHARE + [in_hbm()] * 2,
        out_specs=whole_vmem(),
        scratch_shapes=[
            pltpu.VMEM((1, HEAD), f32),
            pltpu.VMEM(table.shape, f32),
            pltpu.VMEM((SHARE,) + marked.shape, bf16),
            pltpu.SemaphoreType.DMA((2 + SHARE,)),
        ],
        compiler_params=params(24),
        name="query_rotation",
    )(index, held(marked), *shared[1:], held(query_gain.reshape(1, HEAD)), held(table))

    partner, own = attention_call(query_gain, key_gain, shared_rot, kv_parts)
    other = lax.ppermute(partner, "sp", [(i, i ^ 1) for i in range(sp_size)])
    block = own.shape
    partial = pl.pallas_call(
        merge_kernel,
        out_shape=pltpu.HBM(block, bf16),
        in_specs=[pl.BlockSpec(memory_space=pl.ANY)] * 2,
        out_specs=in_hbm(),
        scratch_shapes=[
            pltpu.VMEM(block, bf16), pltpu.VMEM(block, bf16), pltpu.VMEM(block, bf16),
            pltpu.SemaphoreType.DMA((3,)),
        ],
        compiler_params=params(16),
        name="merge_parts",
    )(held(own), other)
    partial = lax.all_to_all(
        partial, ("sp", "tp"), 0, 0, tiled=True, axis_index_groups=owner_groups
    )

    out_rows, model_width = residual.shape
    expert_total = sp_size * tp_size
    flat = routes.T.reshape(-1)
    order = jnp.arange(flat.shape[0], dtype=jnp.int32)
    earlier = (flat[:, None] == flat[None, :]) & (order[None, :] < order[:, None])
    rank = jnp.sum(earlier.astype(jnp.int32), axis=1)
    target = (flat * CAPACITY + rank).reshape(2, out_rows)

    cut = model_width // PARTS
    exchange_rows = expert_total * CAPACITY * PARTS
    middle, outbound = pl.pallas_call(
        middle_kernel,
        out_shape=(
            jax.ShapeDtypeStruct((out_rows, model_width), bf16),
            jax.ShapeDtypeStruct((exchange_rows, cut), bf16),
        ),
        in_specs=[
            whole_vmem(), whole_vmem(), in_hbm(), whole_vmem(),
            whole_vmem(), whole_vmem(), whole_vmem(),
        ],
        out_specs=(whole_vmem(), whole_vmem()),
        scratch_shapes=[
            pltpu.VMEM(out_proj.shape, bf16),
            pltpu.SemaphoreType.DMA((TP,)),
        ],
        compiler_params=params(40),
        name="middle_stream",
    )(
        partial, out_gain.reshape(1, -1), held(out_proj), residual, mid_gain.reshape(1, -1),
        mid_bias.reshape(1, -1), jnp.tile(target, (1, PARTS)),
    )
    arrived = lax.all_to_all(
        outbound.reshape(expert_total, CAPACITY * PARTS, cut), ("sp", "tp"), 0, 0, tiled=True
    )
    hidden_width = expert_gate.shape[2]
    served = pl.pallas_call(
        expert_kernel,
        out_shape=jax.ShapeDtypeStruct((exchange_rows, cut), bf16),
        in_specs=[whole_vmem() for _ in range(4)],
        out_specs=whole_vmem(),
        scratch_shapes=[
            pltpu.VMEM((expert_total * CAPACITY, model_width), bf16),
            pltpu.VMEM((256, 256), bf16),
        ],
        compiler_params=params(40),
        name="expert",
    )(
        arrived.reshape(exchange_rows, cut),
        expert_gate.reshape(model_width, hidden_width),
        expert_up.reshape(model_width, hidden_width),
        expert_down.reshape(hidden_width, model_width),
    )
    returned = lax.all_to_all(
        served.reshape(expert_total, CAPACITY * PARTS, cut), ("sp", "tp"), 0, 0, tiled=True
    )
    return pl.pallas_call(
        final_kernel,
        out_shape=jax.ShapeDtypeStruct((out_rows, model_width), bf16),
        in_specs=[whole_vmem() for _ in range(6)],
        out_specs=whole_vmem(),
        scratch_shapes=[pltpu.VMEM((expert_total * CAPACITY, model_width), bf16)],
        compiler_params=params(40),
        name="final_stream",
    )(
        returned.reshape(exchange_rows, cut), target.T, route_weights, middle,
        final_gain.reshape(1, -1), final_bias.reshape(1, -1),
    )


def solution(mesh):
    rows = P(("sp", "tp"), None)
    experts = P(("sp", "tp"), None, None)
    return jax.shard_map(
        per_device,
        mesh=mesh,
        in_specs=(
            P("sp", "tp"), P("sp", "tp"), P("sp", "tp"), P("sp"), P(), P(), P(), P(), rows, P(),
            P(), rows, rows, experts, experts, experts, P(), P(),
        ),
        out_specs=rows,
        check_vma=False,
    )
```

```python
import numpy as np

import jax
import jax.numpy as jnp
from jax import lax
from jax.experimental import pallas as pl
from jax.experimental.pallas import tpu as pltpu
from jax.sharding import PartitionSpec as P

HEAD = 128
GRID = 64
TP = 4
SHARE = 4
LANES = 128
TILE = 2048
APART = 32768.0
CAPACITY = 4
PARTS = 4
SHARDS = 8
MARKS = 16

eps_norm = 1e-06
alpha_mix = 8.0**0.25
theta_base = 10000.0
score_scale = HEAD**-0.5 * 1.4426950408889634
f32 = jnp.float32
bf16 = jnp.bfloat16


def angle_tables(row_count):
    pair_count = HEAD // 4
    inv_freq = np.power(
        np.float32(theta_base), -np.arange(pair_count, dtype=np.float32) / np.float32(pair_count)
    ).astype(np.float32)

    def both(count):
        angles = (np.arange(count, dtype=np.float32)[:, None] * inv_freq[None, :]).astype(np.float32)
        return np.cos(angles.astype(np.float64)), np.sin(angles.astype(np.float64))

    row_cos, row_sin = both(row_count)
    col_cos, col_sin = both(GRID)
    none_row, none_col = np.zeros_like(row_cos), np.zeros_like(col_cos)
    row_c = np.concatenate([row_cos, none_row, row_cos, none_row], axis=1)
    row_s = np.concatenate([-row_sin, none_row, row_sin, none_row], axis=1)
    col_c = np.concatenate([none_col, col_cos, none_col, col_cos], axis=1)
    col_s = np.concatenate([none_col, -col_sin, none_col, col_sin], axis=1)
    return np.concatenate([row_c, row_s, col_c, col_s], axis=0).astype(np.float32)


def tables_at(table_ref, first, grid_rows):
    row_count = (table_ref.shape[0] - 2 * GRID) // 2

    def table_of(row_first, col_first):
        row_part = table_ref[pl.ds(pl.multiple_of(row_first, 8), grid_rows)]
        col_part = table_ref[col_first : col_first + GRID]
        return (row_part[:, None, :] + col_part[None, :, :]).reshape(grid_rows * GRID, HEAD)

    return (
        table_of(first, 2 * row_count),
        table_of(row_count + first, 2 * row_count + GRID),
    )


def normed_rotated(values, gain_row, cosine, sine):
    inv_rms = lax.rsqrt(jnp.mean(values * values, axis=-1, keepdims=True) + eps_norm)
    values = values * inv_rms * gain_row
    return (values * cosine + pltpu.roll(values, HEAD // 2, 1) * sine).astype(bf16)


def key_kernel(
    index_ref, key_hbm, value_hbm, doc_hbm, gain_hbm, table_hbm, query_hbm, built_ref, lines_ref,
    key_ref, value_ref, doc_ref, gain_ref, table_ref, in_sems,
):
    tok_rows, width = query_hbm.shape
    passing = pltpu.make_async_copy(query_hbm, lines_ref.at[pl.ds(0, tok_rows)], in_sems.at[5])
    pairs = (
        (key_hbm, key_ref), (value_hbm, value_ref), (doc_hbm, doc_ref), (gain_hbm, gain_ref),
        (table_hbm, table_ref),
    )
    arriving = [pltpu.make_async_copy(a, b, in_sems.at[i]) for i, (a, b) in enumerate(pairs)]
    for copy in arriving:
        copy.start()
    passing.start()
    for copy in arriving:
        copy.wait()
    grid_rows = tok_rows // GRID
    cosine, sine = tables_at(table_ref, index_ref[0] * grid_rows, grid_rows)
    rotated = normed_rotated(key_ref[...].astype(f32), gain_ref[...], cosine, sine)
    numbers = lax.broadcasted_iota(jnp.int32, (MARKS, tok_rows), 0)
    documents = doc_ref[...]
    marks = jnp.where(numbers == documents, 1.0, 0.0)
    marks = jnp.where(numbers == MARKS - 1, documents.astype(f32), marks).astype(bf16)
    built_ref[:HEAD, :] = jnp.transpose(rotated.astype(f32)).astype(bf16)
    built_ref[HEAD : HEAD + MARKS, :] = marks
    for g in range(tok_rows // HEAD):
        built_ref[HEAD + MARKS :, g * HEAD : (g + 1) * HEAD] = value_ref[
            g * HEAD : (g + 1) * HEAD, :
        ]
    lines = [
        documents[:, i * width : (i + 1) * width].astype(f32) for i in range(tok_rows // width)
    ]
    lines.append(jnp.zeros((MARKS - len(lines), width), f32))
    lines_ref[tok_rows:, :] = jnp.concatenate(lines, axis=0).astype(bf16)
    passing.wait()


def query_kernel(index_ref, *refs):
    query_hbms = refs[:SHARE]
    (
        gain_hbm, table_hbm, out_ref, gain_ref, table_ref, query_refs, in_sems,
    ) = refs[SHARE:]
    arriving = [
        pltpu.make_async_copy(query_hbm, query_refs.at[i], in_sems.at[2 + i])
        for i, query_hbm in enumerate(query_hbms)
    ] + [
        pltpu.make_async_copy(gain_hbm, gain_ref, in_sems.at[0]),
        pltpu.make_async_copy(table_hbm, table_ref, in_sems.at[1]),
    ]
    for copy in arriving:
        copy.start()
    for copy in arriving:
        copy.wait()
    tok_rows = query_refs.shape[1] - MARKS
    width = query_refs.shape[2]
    grid_rows = tok_rows // GRID
    own = index_ref[0] % SHARE
    numbers = lax.broadcasted_iota(jnp.int32, (LANES, tok_rows), 0).astype(f32)
    for i in range(SHARE):
        query_ref = query_refs.at[i]
        place = own ^ i
        cosine, sine = tables_at(
            table_ref, (index_ref[0] - own + place) * grid_rows, grid_rows
        )
        lines = query_ref[tok_rows:, :].astype(f32)
        documents = jnp.concatenate([lines[k : k + 1] for k in range(tok_rows // width)], axis=1)
        apart = jnp.where(numbers == documents, 0.0, -APART)
        apart = jnp.where(numbers >= MARKS - 2, 0.0, apart)
        apart = jnp.where(numbers == MARKS - 2, documents, apart)
        apart = jnp.transpose(apart).astype(bf16)
        half = 0 if i % 2 else SHARE // 2
        rows = pl.ds(pl.multiple_of((half + place // 2) * tok_rows, tok_rows), tok_rows)
        for h in range(out_ref.shape[0]):
            values = query_ref[:tok_rows, h * HEAD : (h + 1) * HEAD].astype(f32)
            out_ref[h, rows, :HEAD] = normed_rotated(values, gain_ref[...], cosine, sine)
            out_ref[h, rows, HEAD:] = apart


def attention_kernel(query_gain_ref, key_gain_ref, query_ref, *refs):
    kv_refs = refs[:SHARDS]
    refs = refs[SHARDS:]
    (
        partner_ref, own_ref, keys_ref, values_ref, first_ref, last_ref, order_ref, small_ref, acc_ref, total_ref, max_ref,
        key_sems, value_sems,
    ) = refs
    heads, all_rows, depth = query_ref.shape
    tok_rows = keys_ref.shape[2]
    rows = acc_ref.shape[0]
    tile = rows // heads
    marked = HEAD + MARKS
    groups = tok_rows // HEAD
    step = pl.program_id(0)

    @pl.when(step == 0)
    def fetch():
        arriving = []
        for j, kv_ref in enumerate(kv_refs):
            arriving.append(
                pltpu.make_async_copy(
                    kv_ref.at[pl.ds(0, marked)], keys_ref.at[j, pl.ds(0, marked)], key_sems.at[j]
                )
            )
        for j, kv_ref in enumerate(kv_refs):
            for g in range(groups):
                arriving.append(
                    pltpu.make_async_copy(
                        kv_ref.at[pl.ds(marked, HEAD), pl.ds(g * HEAD, HEAD)],
                        values_ref.at[j, pl.ds(g * HEAD, HEAD)],
                        value_sems.at[j * groups + g],
                    )
                )
        for copy in arriving:
            copy.start()
        largest = jnp.max(jnp.abs(query_gain_ref[...])) * jnp.max(jnp.abs(key_gain_ref[...]))
        small_ref[0] = (largest * (HEAD * score_scale * 1.02) < 50.0).astype(jnp.int32)
        for j in range(SHARDS):
            keys_ref[j, marked:, :] = jnp.zeros((depth - marked, tok_rows), bf16)
        for copy in arriving:
            copy.wait()
        for j in range(SHARDS):
            line = keys_ref[j, HEAD:marked, :].astype(f32)
            first_ref[j] = line[MARKS - 1, 0].astype(jnp.int32)
            last_ref[j] = line[MARKS - 1, tok_rows - 1].astype(jnp.int32)

    queries = query_ref[...].reshape(rows, depth)
    low = jnp.int32(1 << 20)
    high = jnp.int32(-1)
    half = all_rows // 2
    for begin in range(0, tile, half):
        top = query_ref[0, begin : begin + 16, HEAD:].astype(f32)
        bottom = query_ref[0, begin + half - 16 : begin + half, HEAD:].astype(f32)
        low = jnp.minimum(low, top[0, MARKS - 2].astype(jnp.int32))
        high = jnp.maximum(high, bottom[15, MARKS - 2].astype(jnp.int32))
    count = jnp.int32(0)
    for j in range(SHARDS):
        order_ref[count] = jnp.int32(j)
        count += ((first_ref[j] <= high) & (last_ref[j] >= low)).astype(jnp.int32)

    acc_ref[...] = jnp.zeros_like(acc_ref)
    total_ref[...] = jnp.zeros_like(total_ref)

    def scores_of(j):
        return jnp.dot(queries, keys_ref[j], preferred_element_type=f32)

    def folded(weights):
        part = weights[:, :LANES]
        for i in range(1, weights.shape[1] // LANES):
            part = part + weights[:, i * LANES : (i + 1) * LANES]
        return part

    @pl.when(small_ref[0] == 1)
    def without_max():
        max_ref[...] = jnp.zeros_like(max_ref)

        def advance(i, unused):
            j = order_ref[i]
            weights = jnp.exp2(scores_of(j) * score_scale)
            total_ref[...] += folded(weights)
            acc_ref[...] += jnp.dot(
                weights.astype(bf16), values_ref[j], preferred_element_type=f32
            )
            return unused

        lax.fori_loop(0, count, advance, 0)

    @pl.when(small_ref[0] == 0)
    def with_max():
        max_ref[...] = jnp.full_like(max_ref, -1e30)

        some_rows = 512

        def advance(i, unused):
            j = order_ref[i]

            def some_of(r, unused):
                mine = pl.ds(pl.multiple_of((r % (tile // some_rows)) * some_rows, some_rows), some_rows)
                held = pl.ds(pl.multiple_of(r * some_rows, some_rows), some_rows)
                part = query_ref[r // (tile // some_rows), mine, :]
                scores = jnp.dot(part, keys_ref[j], preferred_element_type=f32) * score_scale
                old_max = max_ref[held]
                new_max = jnp.maximum(old_max, jnp.max(scores, axis=1, keepdims=True))
                weights = jnp.exp2(scores - new_max[:, :1])
                rescale = jnp.exp2(old_max - new_max)
                max_ref[held] = new_max
                total_ref[held] = total_ref[held] * rescale + folded(weights)
                acc_ref[held] = acc_ref[held] * rescale + jnp.dot(
                    weights.astype(bf16), values_ref[j], preferred_element_type=f32
                )
                return unused

            return lax.fori_loop(0, rows // some_rows, some_of, unused)

        lax.fori_loop(0, count, advance, 0)

    rows_out = LANES
    eye = lax.broadcasted_iota(jnp.int32, (rows_out, LANES), 0) == lax.broadcasted_iota(
        jnp.int32, (rows_out, LANES), 1
    )
    blocks = tile // rows_out
    for h in range(heads):
        for i in range(blocks):
            out_ref = partner_ref.at[i] if i < blocks // 2 else own_ref.at[i - blocks // 2]
            mine = slice(h * tile + i * rows_out, h * tile + (i + 1) * rows_out)
            lanes = slice(h * HEAD, (h + 1) * HEAD)
            total = jnp.sum(total_ref[mine], axis=1, keepdims=True)
            some = total > 0.0
            kept = jnp.where(some, total, 1.0)
            level = jnp.where(some, max_ref[mine] + jnp.log2(kept), -1e30)
            share = 1.0 / kept
            mixed = acc_ref[mine] * share
            out_ref[:rows_out, lanes] = mixed.astype(bf16)
            flat = jnp.sum(jnp.where(eye, level, 0.0), axis=0, keepdims=True)
            top = flat.astype(bf16).astype(f32)
            rest = flat - top
            middle = rest.astype(bf16).astype(f32)
            final = rest - middle
            out_ref[rows_out:, lanes] = jnp.concatenate(
                [top, middle, final, jnp.zeros((13, LANES), f32)], axis=0
            ).astype(bf16)


def layer_norm(stream, gain_row, bias_row):
    center = jnp.mean(stream, axis=-1, keepdims=True)
    spread = jnp.mean(jnp.square(stream - center), axis=-1, keepdims=True)
    return (stream - center) * lax.rsqrt(spread + eps_norm) * gain_row + bias_row


def middle_kernel(
    part_ref, out_gain_ref, proj_ref, residual_ref, gain_ref, bias_ref, target_ref,
    middle_ref, outbound_ref, held_ref, sem_ref,
):
    sources, _, width = part_ref.shape
    copies = [
        pltpu.make_async_copy(
            proj_ref.at[pl.ds(t * width, width)], held_ref.at[pl.ds(t * width, width)], sem_ref.at[t]
        )
        for t in range(TP)
    ]
    for copy in copies:
        copy.start()
    rows = LANES
    heads = width // HEAD
    levels = jnp.sum(part_ref[:, rows:, :].astype(f32), axis=1)
    pieces = [levels[i * TP : (i + 1) * TP] for i in range(sources // TP)]
    highest = pieces[0]
    for piece in pieces[1:]:
        highest = jnp.maximum(highest, piece)
    shares = [jnp.exp2(piece - highest) for piece in pieces]
    whole = shares[0]
    for share in shares[1:]:
        whole = whole + share
    shares = jnp.concatenate([share / whole for share in shares], axis=0)
    columns = []
    for h in range(heads):
        square = jnp.concatenate(
            [
                shares[:, h * HEAD : (h + 1) * HEAD],
                jnp.zeros((LANES - sources, LANES), f32),
            ],
            axis=0,
        )
        columns.append(jnp.transpose(square))
    attended = []
    for t in range(TP):
        for h in range(heads):
            mixed = jnp.zeros((rows, HEAD), f32)
            for i in range(sources // TP):
                source = i * TP + t
                mixed = mixed + columns[h][:, source : source + 1] * part_ref[
                    source, :rows, h * HEAD : (h + 1) * HEAD
                ].astype(f32)
            attended.append(mixed.astype(bf16).astype(f32))
    attention = jnp.concatenate(attended, axis=1)
    mean_square = jnp.mean(attention * attention, axis=1, keepdims=True)
    scaled = (attention * out_gain_ref[...]).astype(bf16)
    projected = jnp.zeros((rows, held_ref.shape[1]), f32)
    for t in range(TP):
        copies[t].wait()
        lanes = slice(t * width, (t + 1) * width)
        projected = projected + jnp.dot(
            scaled[:, lanes], held_ref[lanes, :], preferred_element_type=f32
        )
    projected = projected * lax.rsqrt(mean_square + eps_norm)
    middle = layer_norm(
        alpha_mix * residual_ref[...].astype(f32) + projected, gain_ref[...], bias_ref[...]
    ).astype(bf16)
    middle_ref[...] = middle
    cut = middle.shape[1] // PARTS
    stacked = jnp.concatenate([middle[:, p * cut : (p + 1) * cut] for p in range(PARTS)], axis=0)
    out_rows = outbound_ref.shape[0]
    count = 4
    some = out_rows // count
    for c in range(count):
        row = c * some + lax.broadcasted_iota(jnp.int32, (some, PARTS * rows), 0)
        part = (row // CAPACITY) % PARTS
        slot = (row // (CAPACITY * PARTS)) * CAPACITY + row % CAPACITY
        lane = lax.broadcasted_iota(jnp.int32, (some, PARTS * rows), 1)
        code = jnp.where(part == lane // rows, slot, -1)
        chosen = (code == target_ref[0:1, :]) | (code == target_ref[1:2, :])
        outbound_ref[c * some : (c + 1) * some, :] = jnp.dot(
            jnp.where(chosen, 1.0, 0.0).astype(bf16), stacked, preferred_element_type=f32
        ).astype(bf16)


def swap_matrix(size):
    group = CAPACITY * PARTS
    tiles = size // group
    row = lax.broadcasted_iota(jnp.int32, (size, size), 0)
    col = lax.broadcasted_iota(jnp.int32, (size, size), 1)
    part = row // (tiles * CAPACITY)
    tile = (row // CAPACITY) % tiles
    inner = row % CAPACITY
    return jnp.where(col == tile * group + part * CAPACITY + inner, 1.0, 0.0).astype(bf16)


def expert_kernel(
    arrived_ref, gate_ref, up_ref, down_ref, served_hbm, rows_ref, swap_ref, served_ref, sems
):
    chunk = 256
    chunks = arrived_ref.shape[0] // chunk
    cut = arrived_ref.shape[1]
    some = chunk // PARTS
    swap_ref[...] = swap_matrix(chunk)
    for c in range(chunks):
        sorted_rows = jnp.dot(
            swap_ref[...], arrived_ref[c * chunk : (c + 1) * chunk, :], preferred_element_type=f32
        ).astype(bf16)
        for p in range(PARTS):
            rows_ref[c * some : (c + 1) * some, p * cut : (p + 1) * cut] = sorted_rows[
                p * some : (p + 1) * some
            ]
    rows = rows_ref[...]
    gate = jnp.dot(rows, gate_ref[...], preferred_element_type=f32)
    up = jnp.dot(rows, up_ref[...], preferred_element_type=f32)
    hidden = (gate / (1.0 + jnp.exp(-gate)) * up).astype(bf16)
    rows_ref[...] = jnp.dot(hidden, down_ref[...], preferred_element_type=f32).astype(bf16)
    leaving = []
    for c in range(chunks):
        stacked = jnp.concatenate(
            [
                rows_ref[c * some : (c + 1) * some, p * cut : (p + 1) * cut]
                for p in range(PARTS)
            ],
            axis=0,
        )
        served_ref[c * chunk : (c + 1) * chunk, :] = lax.dot_general(
            swap_ref[...], stacked, (((0,), (0,)), ((), ())), preferred_element_type=f32
        ).astype(bf16)
        mine = pl.ds(c * chunk, chunk)
        leaving.append(
            pltpu.make_async_copy(served_ref.at[mine], served_hbm.at[mine], sems.at[c])
        )
        leaving[-1].start()
    for copy in leaving:
        copy.wait()


def final_kernel(
    returned_ref, target_ref, weight_ref, middle_ref, gain_ref, bias_ref, out_ref, rows_ref
):
    chunk = 256
    chunks = returned_ref.shape[0] // chunk
    cut = returned_ref.shape[1]
    some = chunk // PARTS
    swap = swap_matrix(chunk)
    for c in range(chunks):
        sorted_rows = jnp.dot(
            swap, returned_ref[c * chunk : (c + 1) * chunk, :], preferred_element_type=f32
        ).astype(bf16)
        for p in range(PARTS):
            rows_ref[c * some : (c + 1) * some, p * cut : (p + 1) * cut] = sorted_rows[
                p * some : (p + 1) * some
            ]
    rows = middle_ref.shape[0]
    slot = lax.broadcasted_iota(jnp.int32, (rows, rows_ref.shape[0]), 1)
    chosen = jnp.concatenate(
        [jnp.where(slot == target_ref[:, k : k + 1], 1.0, 0.0) for k in range(2)], axis=0
    ).astype(bf16)
    picked = jnp.dot(chosen, rows_ref[...], preferred_element_type=f32)
    routed = picked[:rows] * weight_ref[:, 0:1] + picked[rows:] * weight_ref[:, 1:2]
    out_ref[...] = layer_norm(
        alpha_mix * middle_ref[...].astype(f32) + routed, gain_ref[...], bias_ref[...]
    ).astype(bf16)


def whole_vmem():
    return pl.BlockSpec(memory_space=pltpu.VMEM)


def in_hbm():
    return pl.BlockSpec(memory_space=pltpu.HBM)


def held(array):
    return pltpu.with_memory_space_constraint(array, pltpu.HBM)


def in_smem():
    return pl.BlockSpec(memory_space=pltpu.SMEM)


def params(mib, grid=0):
    more = {"dimension_semantics": ("arbitrary",)} if grid else {}
    return pltpu.CompilerParams(vmem_limit_bytes=mib << 20, **more)


def merge_kernel(own_ref, other_ref, out_hbm, out_ref, sems):
    blocks = out_ref.shape[0]
    rows = LANES
    heads = out_ref.shape[2] // HEAD
    flats = [
        jnp.sum(ref[:, rows:, :].astype(f32), axis=1) for ref in (own_ref, other_ref)
    ]
    upper = jnp.maximum(flats[0], flats[1])
    parts = [jnp.exp2(flat - upper) for flat in flats]
    both = parts[0] + parts[1]
    flat = upper + jnp.log2(both)
    top = flat.astype(bf16).astype(f32)
    rest = flat - top
    middle = rest.astype(bf16).astype(f32)
    final = rest - middle
    for h in range(heads):
        lanes = slice(h * HEAD, (h + 1) * HEAD)
        shares = jnp.concatenate(
            [(part / both)[:, lanes] for part in parts]
            + [jnp.zeros((LANES - 2 * blocks, LANES), f32)],
            axis=0,
        )
        columns = jnp.transpose(shares)
        for i in range(blocks):
            out_ref[i, :rows, lanes] = (
                own_ref[i, :rows, lanes].astype(f32) * columns[:, i : i + 1]
                + other_ref[i, :rows, lanes].astype(f32) * columns[:, blocks + i : blocks + i + 1]
            ).astype(bf16)
            out_ref[i, rows:, lanes] = jnp.concatenate(
                [
                    top[i : i + 1, lanes], middle[i : i + 1, lanes], final[i : i + 1, lanes],
                    jnp.zeros((13, LANES), f32),
                ],
                axis=0,
            ).astype(bf16)
    leaving = pltpu.make_async_copy(out_ref, out_hbm, sems.at[0])
    leaving.start()
    leaving.wait()


def attention_call(query_gain, key_gain, shared_rot, kv_parts):
    heads, all_rows, depth = shared_rot.shape
    tok_rows = kv_parts[0].shape[1]
    tile = TILE
    width = heads * HEAD
    steps = all_rows // tile
    half_shape = (tile // LANES // 2, LANES + 16, width)
    return pl.pallas_call(
        attention_kernel,
        grid=(steps,),
        out_shape=(jax.ShapeDtypeStruct(half_shape, bf16),) * 2,
        in_specs=[whole_vmem(), whole_vmem(), whole_vmem()] + [pl.BlockSpec(memory_space=pl.ANY)] * SHARDS,
        out_specs=(whole_vmem(), whole_vmem()),
        scratch_shapes=[
            pltpu.VMEM((SHARDS, depth, tok_rows), bf16),
            pltpu.VMEM((SHARDS, tok_rows, HEAD), bf16),
            pltpu.SMEM((SHARDS,), jnp.int32),
            pltpu.SMEM((SHARDS,), jnp.int32),
            pltpu.SMEM((SHARDS,), jnp.int32),
            pltpu.SMEM((1,), jnp.int32),
            pltpu.VMEM((heads * tile, HEAD), f32),
            pltpu.VMEM((heads * tile, HEAD), f32),
            pltpu.VMEM((heads * tile, HEAD), f32),
            pltpu.SemaphoreType.DMA((SHARDS,)),
            pltpu.SemaphoreType.DMA((SHARDS * tok_rows // HEAD,)),
        ],
        compiler_params=params(40, 1),
        name="document_attention",
    )(
        query_gain.reshape(1, HEAD), key_gain.reshape(1, HEAD), shared_rot, *kv_parts,
    )


def per_device(
    queries, key_heads, value_heads, documents, query_gain, key_gain, out_gain, out_proj,
    residual, mid_gain, mid_bias, routes, route_weights, expert_gate, expert_up, expert_down,
    final_gain, final_bias,
):
    tok_rows, width = queries.shape
    heads = width // HEAD
    sp_size = lax.axis_size("sp")
    tp_size = lax.axis_size("tp")
    shards = sp_size // SHARE
    table = jnp.asarray(angle_tables(sp_size * tok_rows // GRID))
    index = lax.axis_index("sp").astype(jnp.int32).reshape(1)
    owner_groups = [
        [(g * SHARE + c + 2 * i) * tp_size + t for i in range(SHARE // 2) for t in range(tp_size)]
        for g in range(shards)
        for c in range(2)
    ]

    kv_rows = 2 * HEAD + MARKS
    kv, marked = pl.pallas_call(
        key_kernel,
        out_shape=(
            jax.ShapeDtypeStruct((kv_rows, tok_rows), bf16),
            jax.ShapeDtypeStruct((tok_rows + MARKS, width), bf16),
        ),
        in_specs=[in_smem()] + [in_hbm()] * 6,
        out_specs=(whole_vmem(), whole_vmem()),
        scratch_shapes=[
            pltpu.VMEM(key_heads.shape, bf16),
            pltpu.VMEM(value_heads.shape, bf16),
            pltpu.VMEM((1, tok_rows), jnp.int32),
            pltpu.VMEM((1, HEAD), f32),
            pltpu.VMEM(table.shape, f32),
            pltpu.SemaphoreType.DMA((6,)),
        ],
        compiler_params=params(16),
        name="key_rotation",
    )(
        index, held(key_heads), held(value_heads), held(documents.reshape(1, tok_rows)),
        held(key_gain.reshape(1, HEAD)), held(table), held(queries),
    )

    def moved(array, dz, dy):
        pairs = []
        for z in range(4):
            for y in range(4):
                for c in range(2):
                    way = 1 - 2 * c
                    goal = ((z + way * dz) % 4) * 8 + ((y + way * dy) % 4) * 2 + c
                    pairs.append((z * 8 + y * 2 + c, goal))
        return lax.ppermute(array, "sp", pairs)

    across = moved(kv, 0, 2)
    after = moved(kv, 1, 0)
    ahead = moved(kv, -1, 0)
    beyond = moved(after, 1, 0)
    after_across = moved(across, 1, 0)
    ahead_across = moved(across, -1, 0)
    beyond_across = moved(after_across, 1, 0)
    kv_parts = [kv, after, ahead, across, beyond, after_across, ahead_across, beyond_across]

    beside = lax.ppermute(marked, "sp", [(i, i ^ 2) for i in range(sp_size)])
    shared = [marked]
    for array in (marked, beside):
        shared.append(lax.ppermute(array, "sp", [(i, i ^ 1) for i in range(sp_size)]))
    shared.insert(2, beside)

    shared_rot = pl.pallas_call(
        query_kernel,
        out_shape=jax.ShapeDtypeStruct((heads, SHARE * tok_rows, 2 * HEAD), bf16),
        in_specs=[in_smem()] + [pl.BlockSpec(memory_space=pl.ANY)] * SHARE + [in_hbm()] * 2,
        out_specs=whole_vmem(),
        scratch_shapes=[
            pltpu.VMEM((1, HEAD), f32),
            pltpu.VMEM(table.shape, f32),
            pltpu.VMEM((SHARE,) + marked.shape, bf16),
            pltpu.SemaphoreType.DMA((2 + SHARE,)),
        ],
        compiler_params=params(24),
        name="query_rotation",
    )(index, *shared, held(query_gain.reshape(1, HEAD)), held(table))

    partner, own = attention_call(query_gain, key_gain, shared_rot, kv_parts)
    other = lax.ppermute(partner, "sp", [(i, i ^ 1) for i in range(sp_size)])
    block = own.shape
    partial = pl.pallas_call(
        merge_kernel,
        out_shape=pltpu.HBM(block, bf16),
        in_specs=[whole_vmem()] * 2,
        out_specs=in_hbm(),
        scratch_shapes=[pltpu.VMEM(block, bf16), pltpu.SemaphoreType.DMA((1,))],
        compiler_params=params(16),
        name="merge_parts",
    )(own, other)
    partial = lax.all_to_all(
        partial, ("sp", "tp"), 0, 0, tiled=True, axis_index_groups=owner_groups
    )

    out_rows, model_width = residual.shape
    expert_total = sp_size * tp_size
    flat = routes.T.reshape(-1)
    order = jnp.arange(flat.shape[0], dtype=jnp.int32)
    earlier = (flat[:, None] == flat[None, :]) & (order[None, :] < order[:, None])
    rank = jnp.sum(earlier.astype(jnp.int32), axis=1)
    target = (flat * CAPACITY + rank).reshape(2, out_rows)

    cut = model_width // PARTS
    exchange_rows = expert_total * CAPACITY * PARTS
    middle, outbound = pl.pallas_call(
        middle_kernel,
        out_shape=(
            jax.ShapeDtypeStruct((out_rows, model_width), bf16),
            jax.ShapeDtypeStruct((exchange_rows, cut), bf16),
        ),
        in_specs=[
            whole_vmem(), whole_vmem(), in_hbm(), whole_vmem(),
            whole_vmem(), whole_vmem(), whole_vmem(),
        ],
        out_specs=(whole_vmem(), whole_vmem()),
        scratch_shapes=[
            pltpu.VMEM(out_proj.shape, bf16),
            pltpu.SemaphoreType.DMA((TP,)),
        ],
        compiler_params=params(40),
        name="middle_stream",
    )(
        partial, out_gain.reshape(1, -1), held(out_proj), residual, mid_gain.reshape(1, -1),
        mid_bias.reshape(1, -1), jnp.tile(target, (1, PARTS)),
    )
    arrived = lax.all_to_all(
        outbound.reshape(expert_total, CAPACITY * PARTS, cut), ("sp", "tp"), 0, 0, tiled=True
    )
    hidden_width = expert_gate.shape[2]
    served = pl.pallas_call(
        expert_kernel,
        out_shape=pltpu.HBM((exchange_rows, cut), bf16),
        in_specs=[whole_vmem() for _ in range(4)],
        out_specs=in_hbm(),
        scratch_shapes=[
            pltpu.VMEM((expert_total * CAPACITY, model_width), bf16),
            pltpu.VMEM((256, 256), bf16),
            pltpu.VMEM((exchange_rows, cut), bf16),
            pltpu.SemaphoreType.DMA((exchange_rows // 256,)),
        ],
        compiler_params=params(40),
        name="expert",
    )(
        arrived.reshape(exchange_rows, cut),
        expert_gate.reshape(model_width, hidden_width),
        expert_up.reshape(model_width, hidden_width),
        expert_down.reshape(hidden_width, model_width),
    )
    returned = lax.all_to_all(
        served.reshape(expert_total, CAPACITY * PARTS, cut), ("sp", "tp"), 0, 0, tiled=True
    )
    return pl.pallas_call(
        final_kernel,
        out_shape=jax.ShapeDtypeStruct((out_rows, model_width), bf16),
        in_specs=[whole_vmem() for _ in range(6)],
        out_specs=whole_vmem(),
        scratch_shapes=[pltpu.VMEM((expert_total * CAPACITY, model_width), bf16)],
        compiler_params=params(40),
        name="final_stream",
    )(
        returned.reshape(exchange_rows, cut), target.T, route_weights, middle,
        final_gain.reshape(1, -1), final_bias.reshape(1, -1),
    )


def solution(mesh):
    rows = P(("sp", "tp"), None)
    experts = P(("sp", "tp"), None, None)
    return jax.shard_map(
        per_device,
        mesh=mesh,
        in_specs=(
            P("sp", "tp"), P("sp", "tp"), P("sp", "tp"), P("sp"), P(), P(), P(), P(), rows, P(),
            P(), rows, rows, experts, experts, experts, P(), P(),
        ),
        out_specs=rows,
        check_vma=False,
    )
```
